32 devices in a mesh: sp: 4 (over y, x), tp: 8 (over z, core).
Axes of the slice: x: 2, y: 2, z: 4, core: 2. Of those that a mesh axis runs over, the one named last changes fastest.
Arguments:
- latent: bfloat16 [2048, 4096], P(('sp', 'tp')), may hold values from -6 to 6
- context: bfloat16 [512, 4096], P('sp'), may hold values from -6 to 6
- condition: float32 [4096], replicated, may hold values from -6 to 6
- context_condition: float32 [4096], replicated, may hold values from -6 to 6
- modulation: bfloat16 [3, 4096, 4096], P(None, 'sp', 'tp'), may hold values from -0.09375 to 0.09375
- query_weight: bfloat16 [4096, 4096], P(None, 'tp'), as said below
- key_weight: bfloat16 [4096, 4096], P(None, 'tp'), as said below
- value_weight: bfloat16 [4096, 4096], P(None, 'tp'), may hold values from -0.09375 to 0.09375
- lambdas: float32 [16], P('tp'), may hold values from 0.3 to 0.8
- context_lift: float32 [16], P('tp'), may hold values from 1.5 to 3
- head_gain: float32 [256], replicated, may hold values from 0.1 to 1.9
- output_weight: bfloat16 [4096, 4096], P('tp'), may hold values from -0.09375 to 0.09375
Outputs:
- result: bfloat16 [2048, 4096], P(('sp', 'tp'))
The draws below stay inside these ranges and needn't reach their ends.
Inputs may be any that keep to these rules, and one draw needn't show every extreme that they name: `query_weight`: entries lie within 200 / sqrt(4096) in magnitude. `key_weight`: entries lie within 6 / sqrt(4096) in magnitude.
All inputs are finite; a program needn't handle non-finite values.
Results may differ from the reference program's by a relative error of at most 0.025.
Values may be sent and summed in bfloat16 or wider, within the bound.
A program may use at most 64 MiB of HBM per device.

```python
import math
import jax
import jax.numpy as jnp
from jax import lax

D = 4096
HEADS = 16
HEAD_DIM = 256
GRID_W = 64
CTX = 512
SEQ = 2048


def common_keys(key):
    gaussian = jax.random.normal(jax.random.fold_in(key, 101), (D, HEADS * HEAD_DIM), jnp.float32)
    return jnp.clip(gaussian, -6.0, 6.0) * D ** (-0.5)


def draw_key_weight(key, part):
    return common_keys(key).astype(jnp.bfloat16)


def draw_query_weight(key, part):
    gaussian = jax.random.normal(jax.random.fold_in(key, 202), (D, HEADS * HEAD_DIM), jnp.float32)
    independent = jnp.clip(gaussian, -6.0, 6.0) * D ** (-0.5)
    return independent.astype(jnp.bfloat16)


def steps_of(rng, extent, shards, low, high):
    gain, own = 1.0, jax.random.fold_in(rng, 6)
    for dim, shards_of in shards:
        heights = jnp.exp(jax.random.uniform(jax.random.fold_in(own, dim), (shards_of,), jnp.float32, low / len(shards), high / len(shards)))
        gain = gain * jnp.repeat(heights, extent[dim] // shards_of).reshape([-1 if axis == dim else 1 for axis in range(len(extent))])
    return gain


def scatter_about(own_key, extent, scale, reach, cuts=(), kind=jnp.bfloat16):
    factor_of = steps_of(own_key, extent, cuts, -0.22, 0.18) if cuts else 1.0
    values = jax.random.normal(own_key, extent, jnp.float32) * scale * factor_of
    return jnp.minimum(jnp.maximum(values, -reach), reach).astype(kind)


def setup_inputs(seed: int = 0) -> dict:
    keys = jax.random.split(jax.random.key(seed), 13)
    latent = scatter_about(keys[0], (SEQ, D), 1.0, 6.0, ((0, 32),))
    context = scatter_about(keys[1], (CTX, D), 1.0, 6.0, ((0, 4),))
    condition = scatter_about(keys[2], (D,), 1.0, 6.0, (), jnp.float32)
    context_condition = scatter_about(keys[3], (D,), 1.0, 6.0, (), jnp.float32)
    modulation = scatter_about(keys[4], (3, D, D), D ** -0.5, 0.09375, ((1, 4), (2, 8)))
    query_weight = draw_query_weight(jax.random.fold_in(keys[12], 71), 0)
    key_weight = draw_key_weight(jax.random.fold_in(keys[12], 71), 0)
    value_weight = scatter_about(keys[7], (D, HEADS * HEAD_DIM), D ** -0.5, 0.09375, ((1, 8),))
    lambdas = jnp.clip(0.3 + 0.5 * jax.random.uniform(keys[8], (HEADS,), jnp.float32) ** steps_of(keys[8], (HEADS,), ((0, 8),), -0.2, 0.2), 0.3, 0.8)
    context_lift = jnp.clip(1.5 + 1.5 * jax.random.uniform(keys[9], (HEADS,), jnp.float32) ** steps_of(keys[9], (HEADS,), ((0, 8),), -0.2, 0.2), 1.5, 3.0)
    head_gain = jnp.clip(1.0 + 0.18 * jax.random.normal(keys[10], (HEAD_DIM,), jnp.float32), 0.1, 1.9)
    output_weight = scatter_about(keys[11], (HEADS * HEAD_DIM, D), (HEADS * HEAD_DIM) ** -0.5, 0.09375, ((0, 8),))
    return {"latent": latent, "context": context, "condition": condition, "context_condition": context_condition, "modulation": modulation, "query_weight": query_weight, "key_weight": key_weight, "value_weight": value_weight, "lambdas": lambdas, "context_lift": context_lift, "head_gain": head_gain, "output_weight": output_weight}


ROPE_BASE = 10000.0
EPSILON = 1e-05

def modulate(tokens_in, offset, scaling):
    values = tokens_in.astype(jnp.float32)
    center = lax.optimization_barrier(jnp.mean(values, axis=-1, keepdims=True))
    spread = lax.optimization_barrier(jnp.mean(jnp.square(values - center), axis=-1, keepdims=True))
    normed = (values - center) * lax.rsqrt(spread + EPSILON)
    return (normed * (1.0 + scaling) + offset).astype(jnp.bfloat16)

def rotate(tensor, places):
    number, head_count, head_width = tensor.shape
    quarter = head_width // 4
    eighth = head_width // 8
    inverse = ROPE_BASE ** (-jnp.arange(eighth, dtype=jnp.float32) / eighth)
    grid_row = (places // GRID_W).astype(jnp.float32)
    grid_col = (places % GRID_W).astype(jnp.float32)
    angles = jnp.stack([grid_row[:, None] * inverse, grid_col[:, None] * inverse], axis=1)
    cosine = jnp.cos(angles)[:, None, None, :, :]
    sine_table = jnp.sin(angles)[:, None, None, :, :]
    pieces = tensor.reshape(number, head_count, 2, 2, quarter)
    first_half = pieces[..., :eighth]
    second = pieces[..., eighth:]
    turned = jnp.concatenate([first_half * cosine - second * sine_table, second * cosine + first_half * sine_table], axis=-1)
    return turned.reshape(number, head_count, head_width)

def reference(latent, context, condition, context_condition, modulation, query_weight, key_weight, value_weight, lambdas, context_lift, head_gain, output_weight):
    silu_pair = jax.nn.silu(jnp.stack([condition, context_condition])).astype(jnp.bfloat16)
    mod_vectors = jnp.einsum('cd,rde->cre', silu_pair.astype(jnp.float32), modulation.astype(jnp.float32))
    normed = modulate(latent, mod_vectors[0, 0], mod_vectors[0, 1])
    normed_context = modulate(context, mod_vectors[1, 0], mod_vectors[1, 1])
    seq_len = latent.shape[0]
    half_width = HEAD_DIM // 2
    scale_factor = half_width ** (-0.5)
    query_raw = jnp.dot(normed, query_weight, preferred_element_type=jnp.float32).astype(jnp.bfloat16)
    key_raw = jnp.dot(normed, key_weight, preferred_element_type=jnp.float32).astype(jnp.bfloat16)
    latent_values = jnp.dot(normed, value_weight, preferred_element_type=jnp.float32).astype(jnp.bfloat16)
    context_keys = jnp.dot(normed_context, key_weight, preferred_element_type=jnp.float32).astype(jnp.bfloat16)
    context_values = jnp.dot(normed_context, value_weight, preferred_element_type=jnp.float32).astype(jnp.bfloat16)
    places = jnp.arange(seq_len, dtype=jnp.int32)
    queries = rotate(query_raw.astype(jnp.float32).reshape(seq_len, HEADS, HEAD_DIM), places).astype(jnp.bfloat16)
    latent_keys = rotate(key_raw.astype(jnp.float32).reshape(seq_len, HEADS, HEAD_DIM), places).astype(jnp.bfloat16)
    all_keys = jnp.concatenate([context_keys.reshape(CTX, HEADS, HEAD_DIM), latent_keys], axis=0)
    all_values = jnp.concatenate([context_values.reshape(CTX, HEADS, HEAD_DIM), latent_values.reshape(seq_len, HEADS, HEAD_DIM)], axis=0)
    key_total = CTX + seq_len
    block_len = math.gcd(seq_len, 1024)

    def one_head(inputs):
        head_queries, head_keys, head_values, head_lambda, head_lift = inputs
        lift_row = jnp.where(jnp.arange(key_total) < CTX, head_lift, 0.0)

        def one_block(block_queries):
            outputs = []
            for map_index in range(2):
                low_col = map_index * half_width
                scores = jnp.dot(block_queries[:, low_col:low_col + half_width], head_keys[:, low_col:low_col + half_width].T, preferred_element_type=jnp.float32) * scale_factor + lift_row
                row_peak = lax.optimization_barrier(jnp.max(scores, axis=1, keepdims=True))
                weights = jnp.exp(scores - row_peak)
                row_sums = lax.optimization_barrier(jnp.sum(weights, axis=1, keepdims=True))
                outputs.append(jnp.dot(weights.astype(jnp.bfloat16), head_values, preferred_element_type=jnp.float32) / row_sums)
            difference = outputs[0] - head_lambda * outputs[1]
            scaled = difference * lax.rsqrt(lax.optimization_barrier(jnp.mean(jnp.square(difference), axis=1, keepdims=True)) + EPSILON) * head_gain
            return scaled.astype(jnp.bfloat16)
        blocks = head_queries.reshape(seq_len // block_len, block_len, HEAD_DIM)
        return lax.map(one_block, blocks).reshape(seq_len, HEAD_DIM)
    heads_out = lax.map(one_head, (queries.transpose(1, 0, 2), all_keys.transpose(1, 0, 2), all_values.transpose(1, 0, 2), lambdas, context_lift))
    attended = heads_out.transpose(1, 0, 2).reshape(seq_len, HEADS * HEAD_DIM)
    mixture = jnp.dot(attended, output_weight, preferred_element_type=jnp.float32)
    return (latent.astype(jnp.float32) + mod_vectors[0, 2] * mixture).astype(jnp.bfloat16)
```

```python
import functools

import jax
import jax.numpy as jnp
import numpy as np
from jax import lax
from jax.experimental import pallas as pl
from jax.experimental.pallas import tpu as pltpu
from jax.sharding import PartitionSpec as P

GRID_W = 64
ROPE_BASE = 10000.0
EPSILON = 1e-05
LOG2E = 1.4426950408889634
ROWS = 16
LANES = 128
UNITS = 4
VMEM_LIMIT = 62 * 1024 * 1024
MESH = pl.DeviceIdType.MESH


def remote(src, dst, send_sem, recv_sem, **where):
    return pltpu.make_async_remote_copy(
        src_ref=src,
        dst_ref=dst,
        send_sem=send_sem,
        recv_sem=recv_sem,
        device_id=where,
        device_id_type=MESH,
    )


def aligned(start, size, unit):
    return pl.ds(pl.multiple_of(start, unit), size)


def block_kernel(
    sp_size,
    tp_size,
    latent,
    context,
    condition,
    context_condition,
    modulation,
    query_weight,
    key_weight,
    value_weight,
    tables,
    lambdas,
    lift,
    gain_in,
    output_weight,
    result,
    tokens,
    context_tokens,
    normed,
    mod_weight,
    wq,
    wk,
    wv,
    weight,
    keys_values,
    queries,
    kv_stage,
    q_stage,
    out_stage,
    attended,
    own,
    stage,
    from_left,
    from_right,
    mod_parts,
    mod_pieces,
    mod_rows,
    vectors_in,
    table,
    cosine,
    sine,
    gain,
    per_head,
    local_sem,
    tok_send,
    tok_recv,
    part_send,
    part_recv,
    piece_send,
    piece_recv,
    kv_send,
    kv_twin,
    kv_recv,
    q_send,
    q_recv,
    out_send,
    out_recv,
    wo_sem,
    head_sem,
    stage_sem,
    left_sem,
    right_sem,
):
    s = lax.axis_index("sp")
    t = lax.axis_index("tp")
    z = lax.div(t, 2)
    c = lax.rem(t, 2)
    twin = t + 1 - 2 * c
    chips = tp_size // 2
    rows, width = latent.shape
    parts = rows // ROWS
    half_rows = rows // 2
    half_parts = parts // 2
    pair = 2 * rows
    block_tokens = tp_size * rows
    ctx_rows = context.shape[0]
    ctx_total = ctx_rows * sp_size
    local = query_weight.shape[1]
    heads = lambdas.shape[0]
    head = local // heads
    half = head // 2
    plane = 2 * heads
    piece = modulation.shape[2]
    depth = modulation.shape[1]
    my_head = lax.rem(s, plane)
    base = s - my_head
    owner_core = lax.div(my_head, heads)
    mine = lax.rem(my_head, heads)
    is_owner = c == owner_core
    ctx_item = 2 * chips

    def load(i, src, dst):
        return pltpu.make_async_copy(src, dst, local_sem.at[i])

    own_slot = tokens.at[aligned(t * rows, rows, ROWS)]
    local_rows = aligned(c * local, local, ROWS)
    here = aligned(s * depth, depth, LANES)
    first_loads = [
        load(0, condition.at[:, here], vectors_in.at[0:1]),
        load(1, context_condition.at[:, here], vectors_in.at[1:2]),
        load(2, modulation, mod_weight),
    ]
    later_loads = [
        load(3, latent, own_slot),
        load(4, context, context_tokens),
        load(5, key_weight, wk),
        load(6, value_weight, wv),
        load(7, tables, table),
        load(8, query_weight, wq),
        load(9, gain_in, gain),
        load(10, output_weight, weight.at[local_rows]),
    ]
    barrier = pltpu.get_barrier_semaphore()
    for k in range(1, tp_size):
        pl.semaphore_signal(
            barrier, inc=1, device_id={"tp": lax.rem(t + k, tp_size)}, device_id_type=MESH
        )
    for k in range(1, sp_size):
        for to in (t, twin):
            pl.semaphore_signal(
                barrier,
                inc=1,
                device_id={"sp": lax.rem(s + k, sp_size), "tp": to},
                device_id_type=MESH,
            )
    for copy in first_loads + later_loads[:-1]:
        copy.start()
    for g in range(heads):
        per_head[c, 2 * g : 2 * g + 1, :] = jnp.full((1, LANES), lambdas[g], jnp.float32)
        per_head[c, 2 * g + 1 : 2 * g + 2, :] = jnp.full((1, LANES), lift[g], jnp.float32)
    pl.semaphore_wait(barrier, tp_size - 1 + 2 * (sp_size - 1))

    def token_copy(kind, b, core, part, mine_first=False):
        slot = 2 * b + core
        place = tokens.at[aligned(slot * rows + part * ROWS, ROWS, ROWS)]
        to = (t + 2, t - 2, twin)[kind]
        return remote(
            latent.at[aligned(part * ROWS, ROWS, ROWS)] if mine_first else place,
            place,
            tok_send.at[kind, parts * b + part],
            tok_recv.at[parts * slot + part],
            tp=to,
        )

    def send_mine(part):
        @pl.when(z + 1 < chips)
        def _():
            token_copy(0, z, c, part, True).start()

        @pl.when(z > 0)
        def _():
            token_copy(1, z, c, part, True).start()

        token_copy(2, z, c, part, True).start()

    for part in range(parts - 1):
        send_mine(part)

    first_loads[0].wait()
    first_loads[1].wait()
    v = vectors_in[...]
    v = v / (1.0 + jnp.exp(-v))
    which = lax.broadcasted_iota(jnp.int32, (ROWS, depth), 0)
    vectors = jnp.where(
        which == 0,
        jnp.broadcast_to(v[0:1], (ROWS, depth)),
        jnp.broadcast_to(v[1:2], (ROWS, depth)),
    ).astype(jnp.bfloat16)
    first_loads[2].wait()
    for r in range(3):
        found = jnp.dot(vectors, mod_weight[r], preferred_element_type=jnp.float32)
        mod_parts[s, 2 * r : 2 * r + 2, :] = found[0:2]
    mod_parts[s, 6:8, :] = jnp.zeros((2, piece), jnp.float32)

    def part_copy(k, owner):
        return remote(
            mod_parts.at[owner],
            mod_parts.at[owner],
            part_send.at[k],
            part_recv.at[owner],
            sp=lax.rem(s + k, sp_size),
        )

    def piece_copy(k, owner):
        return remote(
            mod_pieces.at[owner],
            mod_pieces.at[owner],
            piece_send.at[k],
            piece_recv.at[owner],
            tp=lax.rem(t + k, tp_size),
        )

    def head_copy(core):
        return remote(per_head.at[core], per_head.at[core], head_sem.at[0], head_sem.at[1], tp=twin)

    def weight_copy(core):
        return remote(
            output_weight,
            weight.at[aligned(core * local, local, ROWS)],
            wo_sem.at[0],
            wo_sem.at[1],
            tp=twin,
        )

    for k in range(1, sp_size):
        part_copy(k, s).start()
    head_copy(c).start()
    for k in range(1, sp_size):
        part_copy(k, lax.rem(s + k, sp_size)).wait_recv()
    total = mod_parts[0]
    for i in range(1, sp_size):
        total = total + mod_parts[i]
    mod_pieces[t] = total
    for k in range(1, tp_size):
        piece_copy(k, t).start()
    send_mine(parts - 1)
    later_loads[-1].start()
    weight_copy(c).start()

    def forward(d, part):
        left = z - d
        right = z + d

        @pl.when(left >= 0)
        def _():
            token_copy(2, left, c, part).wait_recv()

            @pl.when(z + 1 < chips)
            def _():
                token_copy(0, left, c, part).start()

            token_copy(2, left, c, part).start()

        @pl.when(right < chips)
        def _():
            token_copy(2, right, c, part).wait_recv()

            @pl.when(z > 0)
            def _():
                token_copy(1, right, c, part).start()

            token_copy(2, right, c, part).start()

    for part in range(parts - 1):
        forward(1, part)

    grid_rows = block_tokens // GRID_W
    all_rows = table.shape[1] - GRID_W
    later_loads[4].wait()
    is_row = lax.broadcasted_iota(jnp.int32, (GRID_W, half), 1) < half // 2
    for kind, into in enumerate((cosine, sine)):
        by_col = table[kind, all_rows:, :]
        for r in range(grid_rows):
            by_row = table[kind, pl.ds(s * grid_rows + r, 1), :]
            into[r * GRID_W : (r + 1) * GRID_W, :] = jnp.where(is_row, by_row, by_col)

    for k in range(1, tp_size):
        piece_copy(k, lax.rem(t + k, tp_size)).wait_recv()
    for i in range(tp_size):
        found = mod_pieces[i]
        mod_rows[0:2, i * piece : (i + 1) * piece] = found[0:2]
        mod_rows[2:4, i * piece : (i + 1) * piece] = 1.0 + found[2:4]
        mod_rows[4:6, i * piece : (i + 1) * piece] = found[4:6]

    tiles = width // LANES

    def normalise(pieces, row):
        def tile(ref, start, count, i):
            x = ref[aligned(start, count, ROWS), i * LANES : (i + 1) * LANES]
            return x.astype(jnp.float32)

        to = 0
        for ref, start, count in pieces:
            sums = tile(ref, start, count, 0)
            for i in range(1, tiles):
                sums = sums + tile(ref, start, count, i)
            center = jnp.sum(sums, axis=1, keepdims=True) * (1.0 / width)
            squares = jnp.zeros((count, LANES), jnp.float32)
            for i in range(tiles):
                x = tile(ref, start, count, i) - center
                squares = squares + x * x
            spread = jnp.sum(squares, axis=1, keepdims=True) * (1.0 / width)
            inverse = lax.rsqrt(spread + EPSILON)
            for i in range(tiles):
                cols = slice(i * LANES, (i + 1) * LANES)
                x = (tile(ref, start, count, i) - center) * inverse
                y = x * mod_rows[2 + row : 3 + row, cols] + mod_rows[row : row + 1, cols]
                normed[to : to + count, cols] = y.astype(jnp.bfloat16)
            to += count

    def kv_place(owner, item):
        return aligned(ctx_total + owner * block_tokens + item * rows, rows, ROWS)

    def ctx_place(owner):
        return aligned(owner * ctx_rows, ctx_rows, ROWS)

    def stage_place(item):
        return aligned(item * rows, rows, ROWS)

    ctx_stage = pl.ds(block_tokens, ctx_rows)

    def kv_copy(k, owner, item, is_context):
        to = lax.rem(s + k, sp_size)
        return remote(
            kv_stage.at[lax.rem(to, heads), ctx_stage if is_context else stage_place(item)],
            keys_values.at[ctx_place(owner) if is_context else kv_place(owner, item)],
            kv_send.at[k, item],
            kv_recv.at[owner, item],
            sp=to,
        )

    def wanted(k):
        to = lax.rem(s + k, sp_size)
        return lax.div(lax.rem(to, plane), heads) == c

    def twin_copy(owner, item, is_context):
        place = keys_values.at[ctx_place(owner) if is_context else kv_place(owner, item)]
        return remote(place, place, kv_twin.at[owner, item], kv_recv.at[owner, item], tp=twin)

    def hand_out(keys, values, item, is_context):
        place = ctx_stage if is_context else stage_place(item)
        for g in range(heads):
            kv_stage[g, place, :head] = keys[:, g * head : (g + 1) * head]
            kv_stage[g, place, head:] = values[:, g * head : (g + 1) * head]
        for k in range(1, sp_size):

            @pl.when(wanted(k))
            def _():
                kv_copy(k, s, item, is_context).start()

        @pl.when(is_owner)
        def _():
            to = ctx_place(s) if is_context else kv_place(s, item)
            keys_values[to, :] = kv_stage[mine, place, :]
            twin_copy(s, item, is_context).start()

    def pass_on(item, is_context):
        @pl.when(is_owner)
        def _():
            for k in range(1, sp_size):
                owner = lax.rem(s + k, sp_size)
                kv_copy(k, owner, item, is_context).wait_recv()
                twin_copy(owner, item, is_context).start()

    def q_copy(g, rel, source, item):
        core = c + rel - 2 * c * rel
        b = lax.div(item, 2)
        side = lax.rem(item, 2)
        return remote(
            q_stage.at[g, aligned(item * rows + core * half_rows, half_rows, ROWS)],
            queries.at[b, aligned(source * rows + side * half_rows, half_rows, ROWS)],
            q_send.at[2 * g + rel, item],
            q_recv.at[source, item],
            sp=base + c * heads + g,
            tp=twin if rel else t,
        )

    def out_copy(b, k, index):
        to = lax.rem(my_head + k, plane)
        return remote(
            out_stage.at[b, aligned(to * rows, rows, ROWS)],
            attended.at[b, index],
            out_send.at[b, k],
            out_recv.at[b, index],
            sp=base + to,
        )

    quarter = half // 4
    lane = lax.broadcasted_iota(jnp.int32, (rows, half), 1)
    low = lax.rem(lane, 2 * quarter) < quarter

    def turn(raw, b, side):
        def of(ref):
            return jnp.concatenate(
                [
                    ref[aligned(b * pair + core * rows + side * half_rows, half_rows, ROWS), :]
                    for core in range(2)
                ],
                axis=0,
            )

        cos = of(cosine)
        sin = of(sine)
        found = []
        for i in range(local // half):
            v = raw[:, i * half : (i + 1) * half].astype(jnp.bfloat16).astype(jnp.float32)
            other = jnp.where(low, pltpu.roll(v, half - quarter, 1), pltpu.roll(v, quarter, 1))
            found.append((v * cos + other * sin).astype(jnp.bfloat16))
        return jnp.concatenate(found, axis=1)

    def process(b, side):
        item = 2 * b + side
        for i in range(half_parts):
            token_copy(2, b, 1 - c, side * half_parts + i).wait_recv()
        normalise(
            [(tokens, (2 * b + core) * rows + side * half_rows, half_rows) for core in range(2)], 0
        )
        x = normed[:rows, :]
        hand_out(
            turn(jnp.dot(x, wk[...], preferred_element_type=jnp.float32), b, side),
            jnp.dot(x, wv[...], preferred_element_type=jnp.float32).astype(jnp.bfloat16),
            item,
            False,
        )
        turned = turn(jnp.dot(x, wq[...], preferred_element_type=jnp.float32), b, side)
        for g in range(heads):
            q_stage[g, stage_place(item), :] = turned[:, g * head : (g + 1) * head]
            for rel in range(2):
                if rel:
                    q_copy(g, rel, my_head, item).start()
                else:

                    @pl.when(c * heads + g != my_head)
                    def _():
                        q_copy(g, rel, my_head, item).start()

                    @pl.when(c * heads + g == my_head)
                    def _():
                        queries[
                            b, aligned(my_head * rows + side * half_rows, half_rows, ROWS), :
                        ] = q_stage[g, aligned(item * rows + c * half_rows, half_rows, ROWS), :]

    for i in (1, 2, 3):
        later_loads[i].wait()
    step_rows = min(ctx_rows, 2 * ROWS)

    def context_group(i, carry):
        normalise_context(i)
        return carry

    def normalise_context(i):
        start = i * step_rows
        x = context_tokens[aligned(start, step_rows, ROWS), :].astype(jnp.float32)
        x = x - jnp.sum(x, axis=1, keepdims=True) * (1.0 / width)
        spread = jnp.sum(x * x, axis=1, keepdims=True) * (1.0 / width)
        y = x * lax.rsqrt(spread + EPSILON) * mod_rows[3:4, :] + mod_rows[1:2, :]
        normed[aligned(start, step_rows, ROWS), :] = y.astype(jnp.bfloat16)

    lax.fori_loop(0, ctx_rows // step_rows, context_group, 0)
    hand_out(
        jnp.dot(normed[:ctx_rows, :], wk[...], preferred_element_type=jnp.float32).astype(
            jnp.bfloat16
        ),
        jnp.dot(normed[:ctx_rows, :], wv[...], preferred_element_type=jnp.float32).astype(
            jnp.bfloat16
        ),
        ctx_item,
        True,
    )
    forward(1, parts - 1)
    later_loads[0].wait()
    later_loads[5].wait()

    flip = jnp.where(2 * z >= chips, 0, 1)

    def step(j, last):
        d = lax.div(j, 4)
        turn_of = lax.rem(lax.div(j, 2), 2)
        side = lax.rem(j, 2)
        pick = turn_of + flip - 2 * turn_of * flip
        b = z - d + 2 * d * pick
        valid = (b >= 0) & (b < chips) & (d + 1 > turn_of)

        @pl.when(((d == 1) & (side == 0)) | ((d >= 3) & (turn_of == 0)))
        def _():
            which_half = jnp.where(d == 1, turn_of, side)
            for i in range(half_parts):
                forward(jnp.where(d == 1, 2, d), which_half * half_parts + i)

        @pl.when(valid)
        def _():
            process(b, side)

            @pl.when(j > 0)
            def _():
                pass_on(last, False)

        @pl.when(j == 0)
        def _():
            pass_on(ctx_item, True)

        return jnp.where(valid, 2 * b + side, last)

    last = lax.fori_loop(0, 4 * chips, step, 2 * z)
    pass_on(last, False)

    @pl.when(jnp.logical_not(is_owner))
    def _():
        def take(i, carry):
            twin_copy(lax.div(i, 2 * chips), lax.rem(i, 2 * chips), False).wait_recv()
            return carry

        lax.fori_loop(0, sp_size * 2 * chips, take, 0)

        def take_context(i, carry):
            twin_copy(i, ctx_item, True).wait_recv()
            return carry

        lax.fori_loop(0, sp_size, take_context, 0)

    head_copy(1 - c).wait_recv()
    weight_copy(1 - c).wait_recv()
    later_loads[6].wait()
    later_loads[7].wait()

    tile = plane * rows
    factor = half ** (-0.5) * LOG2E
    weight_of_second = per_head[owner_core, pl.ds(2 * mine, 1), :][:, 0:1]
    raised = per_head[owner_core, pl.ds(2 * mine + 1, 1), :][:, 0:1] * LOG2E

    def attention(b):
        for k in range(plane):
            source = lax.rem(my_head + k, plane)

            @pl.when(jnp.logical_or(k > 0, jnp.logical_not(is_owner)))
            def _():
                for side in range(2):
                    q_copy(0, 0, source, 2 * b + side).wait_recv()

        outs = []
        for m in range(2):
            scores = lax.dot_general(
                queries[b, :, m * half : (m + 1) * half],
                keys_values[:, m * half : (m + 1) * half],
                (((1,), (1,)), ((), ())),
                preferred_element_type=jnp.float32,
            )
            scores = jnp.concatenate(
                [scores[:, :ctx_total] * factor + raised, scores[:, ctx_total:] * factor], axis=1
            )
            weights = jnp.exp2(scores - jnp.max(scores, axis=1, keepdims=True))
            sums = jnp.sum(weights, axis=1, keepdims=True)
            outs.append(
                jnp.dot(
                    weights.astype(jnp.bfloat16),
                    keys_values[:, head:],
                    preferred_element_type=jnp.float32,
                )
                / sums
            )
        diff = outs[0] - weight_of_second * outs[1]
        mean = jnp.sum(diff * diff, axis=1, keepdims=True) * (1.0 / head)
        out_stage[b, :, :] = (diff * lax.rsqrt(mean + EPSILON) * gain[...]).astype(jnp.bfloat16)
        for k in range(1, plane):
            out_copy(b, k, my_head).start()
        attended[b, my_head] = out_stage[b, aligned(my_head * rows, rows, ROWS), :]

    span = width // UNITS
    at_end = (z == 0) | (z + 1 == chips)

    def right_copy(u):
        return remote(stage.at[u], from_left.at[u], stage_sem.at[u], left_sem.at[u], tp=t + 2)

    def left_copy(u):
        return remote(stage.at[u], from_right.at[u], stage_sem.at[u], right_sem.at[u], tp=t - 2)

    def project(b):
        for k in range(1, plane):
            out_copy(b, k, lax.rem(my_head + k, plane)).wait_recv()
        x = jnp.concatenate([attended[b, g] for g in range(plane)], axis=1)
        for n in range(UNITS):
            u = b * UNITS + n
            found = jnp.dot(
                x, weight[:, n * span : (n + 1) * span], preferred_element_type=jnp.float32
            )
            own[u] = found

            @pl.when(at_end & (b != z))
            def _():
                stage[u] = found.astype(jnp.bfloat16)

                @pl.when(z == 0)
                def _():
                    right_copy(u).start()

                @pl.when(z > 0)
                def _():
                    left_copy(u).start()

    near = jnp.minimum(z, chips - 1 - z)
    far = jnp.maximum(z, chips - 1 - z)

    def block_of(i):
        r = i - (far - near)
        single = r < 0
        dist = jnp.where(single, far - i, near - lax.div(jnp.maximum(r, 0), 2))
        turn_of = jnp.where(single, 0, lax.rem(jnp.maximum(r, 0), 2))
        pick = turn_of + flip - 2 * turn_of * flip
        return z - dist + 2 * dist * pick

    def attend_step(i, carry):
        @pl.when(i < chips)
        def _():
            attention(block_of(i))

        @pl.when(i > 0)
        def _():
            project(block_of(i - 1))

        return carry

    lax.fori_loop(0, chips + 1, attend_step, 0)

    hop = 2

    def combine_step(i, carry):
        q = i - hop * (chips - 1 - z)
        b = lax.div(jnp.maximum(q, 0), UNITS)

        @pl.when((q >= 0) & (b < z))
        def _():
            left_copy(q).wait_recv()
            stage[q] = (own[q] + from_right[q].astype(jnp.float32)).astype(jnp.bfloat16)
            left_copy(q).start()

        p = i - hop * z
        e = chips - 1 - lax.div(jnp.maximum(p, 0), UNITS)
        u = e * UNITS + lax.rem(jnp.maximum(p, 0), UNITS)

        @pl.when((p >= 0) & (e > z))
        def _():
            right_copy(u).wait_recv()
            stage[u] = (own[u] + from_left[u].astype(jnp.float32)).astype(jnp.bfloat16)
            right_copy(u).start()

        return carry

    @pl.when(jnp.logical_not(at_end))
    def _():
        lax.fori_loop(0, (chips - 1) * UNITS + hop * (chips - 1), combine_step, 0)

    for n in range(UNITS):
        u = z * UNITS + n
        cols = slice(n * span, (n + 1) * span)

        @pl.when(z > 0)
        def _():
            right_copy(u).wait_recv()
            own[u] = own[u] + from_left[u].astype(jnp.float32)

        @pl.when(z + 1 < chips)
        def _():
            left_copy(u).wait_recv()
            own[u] = own[u] + from_right[u].astype(jnp.float32)

        result[:, cols] = (
            tokens[aligned(t * rows, rows, ROWS), cols].astype(jnp.float32)
            + mod_rows[4:5, cols] * own[u]
        ).astype(jnp.bfloat16)

    def sent_stage(u, carry):
        @pl.when(lax.div(u, UNITS) != z)
        def _():
            left_copy(u).wait_send()

        return carry

    lax.fori_loop(0, UNITS * chips, sent_stage, 0)

    def sent_block(b, carry):
        for k in range(1, plane):
            out_copy(b, k, my_head).wait_send()
        for part in range(parts):

            @pl.when((b <= z) & (z + 1 < chips))
            def _():
                token_copy(0, b, c, part).wait_send()

            @pl.when((b >= z) & (z > 0))
            def _():
                token_copy(1, b, c, part).wait_send()

            token_copy(2, b, c, part).wait_send()
        return carry

    lax.fori_loop(0, chips, sent_block, 0)

    def sent_item(item, carry):
        for g in range(heads):
            q_copy(g, 1, my_head, item).wait_send()

            @pl.when(c * heads + g != my_head)
            def _():
                q_copy(g, 0, my_head, item).wait_send()

        for k in range(1, sp_size):

            @pl.when(wanted(k))
            def _():
                kv_copy(k, s, item, False).wait_send()

        @pl.when(is_owner)
        def _():
            for k in range(sp_size):
                twin_copy(k, item, False).wait_send()

        return carry

    lax.fori_loop(0, 2 * chips, sent_item, 0)
    for k in range(1, sp_size):
        part_copy(k, s).wait_send()

        @pl.when(wanted(k))
        def _():
            kv_copy(k, s, ctx_item, True).wait_send()

    @pl.when(is_owner)
    def _():
        for k in range(sp_size):
            twin_copy(k, ctx_item, True).wait_send()

    for k in range(1, tp_size):
        piece_copy(k, t).wait_send()
    head_copy(c).wait_send()
    weight_copy(c).wait_send()


def tables(grid_rows, half):
    quarter = half // 4
    inverse = (ROPE_BASE ** (-np.arange(quarter) / quarter)).astype(np.float32)
    sign = np.where(np.arange(half) % (2 * quarter) < quarter, -1.0, 1.0)
    places = np.concatenate([np.arange(grid_rows), np.arange(GRID_W)]).astype(np.float32)
    angles = (places[:, None] * np.tile(inverse, 4)).astype(np.float64)
    return np.stack([np.cos(angles), np.sin(angles) * sign]).astype(np.float32)


def shards(
    sp_size,
    tp_size,
    latent,
    context,
    condition,
    context_condition,
    modulation,
    query_weight,
    key_weight,
    value_weight,
    lambdas,
    context_lift,
    head_gain,
    output_weight,
):
    rows, width = latent.shape
    chips = tp_size // 2
    local = query_weight.shape[1]
    heads = lambdas.shape[0]
    head = local // heads
    half = head // 2
    plane = 2 * heads
    block_tokens = rows * tp_size
    ctx_rows = context.shape[0]
    piece = modulation.shape[2]
    depth = modulation.shape[1]
    parts = rows // ROWS
    table = tables(sp_size * block_tokens // GRID_W, half)
    vmem = pl.BlockSpec(memory_space=pltpu.VMEM)
    smem = pl.BlockSpec(memory_space=pltpu.SMEM)
    anywhere = pl.BlockSpec(memory_space=pl.ANY)
    bf16, f32 = jnp.bfloat16, jnp.float32
    dma = pltpu.SemaphoreType.DMA
    units = (UNITS * chips, rows, width // UNITS)
    return pl.pallas_call(
        functools.partial(block_kernel, sp_size, tp_size),
        out_shape=jax.ShapeDtypeStruct((rows, width), bf16),
        in_specs=[anywhere] * 9 + [smem] * 2 + [anywhere] * 2,
        out_specs=vmem,
        scratch_shapes=[
            pltpu.VMEM((block_tokens, width), bf16),
            pltpu.VMEM(context.shape, bf16),
            pltpu.VMEM((max(rows, ctx_rows), width), bf16),
            pltpu.VMEM(modulation.shape, bf16),
            pltpu.VMEM((width, local), bf16),
            pltpu.VMEM((width, local), bf16),
            pltpu.VMEM((width, local), bf16),
            pltpu.VMEM((2 * local, width), bf16),
            pltpu.VMEM((sp_size * (ctx_rows + block_tokens), 2 * head), bf16),
            pltpu.VMEM((chips, plane * rows, head), bf16),
            pltpu.VMEM((heads, block_tokens + ctx_rows, 2 * head), bf16),
            pltpu.VMEM((heads, block_tokens, head), bf16),
            pltpu.VMEM((chips, plane * rows, head), bf16),
            pltpu.VMEM((chips, plane, rows, head), bf16),
            pltpu.VMEM(units, f32),
            pltpu.VMEM(units, bf16),
            pltpu.VMEM(units, bf16),
            pltpu.VMEM(units, bf16),
            pltpu.VMEM((sp_size, 8, piece), f32),
            pltpu.VMEM((tp_size, 8, piece), f32),
            pltpu.VMEM((8, width), f32),
            pltpu.VMEM((2, depth), f32),
            pltpu.VMEM(table.shape, f32),
            pltpu.VMEM((block_tokens, half), f32),
            pltpu.VMEM((block_tokens, half), f32),
            pltpu.VMEM((1, head), f32),
            pltpu.VMEM((2, 8, LANES), f32),
            dma((11,)),
            dma((3, parts * chips)),
            dma((parts * tp_size,)),
            dma((sp_size,)),
            dma((sp_size,)),
            dma((tp_size,)),
            dma((tp_size,)),
            dma((sp_size, 2 * chips + 1)),
            dma((sp_size, 2 * chips + 1)),
            dma((sp_size, 2 * chips + 1)),
            dma((2 * heads, 2 * chips)),
            dma((plane, 2 * chips)),
            dma((chips, plane)),
            dma((chips, plane)),
            dma((2,)),
            dma((2,)),
            dma((UNITS * chips,)),
            dma((UNITS * chips,)),
            dma((UNITS * chips,)),
        ],
        compiler_params=pltpu.CompilerParams(
            collective_id=0, has_side_effects=True, vmem_limit_bytes=VMEM_LIMIT
        ),
        name="block",
    )(
        latent,
        context,
        condition.reshape(1, -1),
        context_condition.reshape(1, -1),
        modulation,
        query_weight,
        key_weight,
        value_weight,
        table,
        lambdas,
        context_lift,
        head_gain.reshape(1, -1),
        output_weight,
    )


def solution(mesh):
    in_specs = (
        P(("sp", "tp"), None),
        P("sp", None),
        P(),
        P(),
        P(None, "sp", "tp"),
        P(None, "tp"),
        P(None, "tp"),
        P(None, "tp"),
        P("tp"),
        P("tp"),
        P(),
        P("tp", None),
    )
    out_specs = P(("sp", "tp"), None)
    body = functools.partial(shards, mesh.shape["sp"], mesh.shape["tp"])
    return jax.shard_map(body, mesh=mesh, in_specs=in_specs, out_specs=out_specs, check_vma=False)
```

```python
import functools

import jax
import jax.numpy as jnp
import numpy as np
from jax import lax
from jax.experimental import pallas as pl
from jax.experimental.pallas import tpu as pltpu
from jax.sharding import PartitionSpec as P

GRID_W = 64
ROPE_BASE = 10000.0
EPSILON = 1e-05
LOG2E = 1.4426950408889634
ROWS = 16
LANES = 128
UNITS = 4
VMEM_LIMIT = 62 * 1024 * 1024
MESH = pl.DeviceIdType.MESH


def remote(src, dst, send_sem, recv_sem, **where):
    return pltpu.make_async_remote_copy(
        src_ref=src,
        dst_ref=dst,
        send_sem=send_sem,
        recv_sem=recv_sem,
        device_id=where,
        device_id_type=MESH,
    )


def aligned(start, size, unit):
    return pl.ds(pl.multiple_of(start, unit), size)


def block_kernel(
    sp_size,
    tp_size,
    latent,
    context,
    condition,
    context_condition,
    modulation,
    query_weight,
    key_weight,
    value_weight,
    tables,
    lambdas,
    lift,
    gain_in,
    output_weight,
    result,
    tokens,
    context_tokens,
    normed,
    mod_weight,
    wq,
    wk,
    wv,
    weight,
    keys_values,
    queries,
    kv_stage,
    q_stage,
    out_stage,
    attended,
    own,
    stage,
    from_left,
    from_right,
    mod_parts,
    mod_pieces,
    mod_rows,
    vectors_in,
    table,
    cosine,
    sine,
    gain,
    per_head,
    held,
    held_peak,
    held_sums,
    local_sem,
    tok_send,
    tok_recv,
    part_send,
    part_recv,
    piece_send,
    piece_recv,
    kv_send,
    kv_twin,
    kv_recv,
    kv_pass,
    q_send,
    q_recv,
    out_send,
    out_recv,
    wo_sem,
    head_sem,
    stage_sem,
    left_sem,
    right_sem,
):
    s = lax.axis_index("sp")
    t = lax.axis_index("tp")
    z = lax.div(t, 2)
    c = lax.rem(t, 2)
    twin = t + 1 - 2 * c
    chips = tp_size // 2
    rows, width = latent.shape
    parts = rows // ROWS
    half_rows = rows // 2
    half_parts = parts // 2
    pair = 2 * rows
    block_tokens = tp_size * rows
    ctx_rows = context.shape[0]
    ctx_total = ctx_rows * sp_size
    local = query_weight.shape[1]
    heads = lambdas.shape[0]
    head = local // heads
    half = head // 2
    plane = 2 * heads
    piece = modulation.shape[2]
    depth = modulation.shape[1]
    my_head = lax.rem(s, plane)
    base = s - my_head
    owner_core = lax.div(my_head, heads)
    mine = lax.rem(my_head, heads)
    is_owner = c == owner_core
    ctx_item = 2 * chips

    def load(i, src, dst):
        return pltpu.make_async_copy(src, dst, local_sem.at[i])

    own_slot = tokens.at[aligned(t * rows, rows, ROWS)]
    local_rows = aligned(c * local, local, ROWS)
    here = aligned(s * depth, depth, LANES)
    first_loads = [
        load(0, condition.at[:, here], vectors_in.at[0:1]),
        load(1, context_condition.at[:, here], vectors_in.at[1:2]),
        load(2, modulation, mod_weight),
    ]
    later_loads = [
        load(3, latent, own_slot),
        load(4, context, context_tokens),
        load(5, key_weight, wk),
        load(6, value_weight, wv),
        load(7, tables, table),
        load(8, query_weight, wq),
        load(9, gain_in, gain),
        load(10, output_weight, weight.at[local_rows]),
    ]
    barrier = pltpu.get_barrier_semaphore()
    for k in range(1, tp_size):
        pl.semaphore_signal(
            barrier, inc=1, device_id={"tp": lax.rem(t + k, tp_size)}, device_id_type=MESH
        )
    for k in range(1, sp_size):
        for to in (t, twin):
            pl.semaphore_signal(
                barrier,
                inc=1,
                device_id={"sp": lax.rem(s + k, sp_size), "tp": to},
                device_id_type=MESH,
            )
    for copy in first_loads + later_loads[:-1]:
        copy.start()
    for g in range(heads):
        per_head[c, 2 * g : 2 * g + 1, :] = jnp.full((1, LANES), lambdas[g], jnp.float32)
        per_head[c, 2 * g + 1 : 2 * g + 2, :] = jnp.full((1, LANES), lift[g], jnp.float32)
    pl.semaphore_wait(barrier, tp_size - 1 + 2 * (sp_size - 1))

    def token_copy(kind, b, core, part, mine_first=False):
        slot = 2 * b + core
        place = tokens.at[aligned(slot * rows + part * ROWS, ROWS, ROWS)]
        to = (t + 2, t - 2, twin)[kind]
        return remote(
            latent.at[aligned(part * ROWS, ROWS, ROWS)] if mine_first else place,
            place,
            tok_send.at[kind, 0 if kind == 2 else b],
            tok_recv.at[parts * slot + part],
            tp=to,
        )

    def send_mine(part):
        @pl.when(z + 1 < chips)
        def _():
            token_copy(0, z, c, part, True).start()

        @pl.when(z > 0)
        def _():
            token_copy(1, z, c, part, True).start()

        token_copy(2, z, c, part, True).start()

    for part in range(half_parts):
        send_mine(part)

    first_loads[0].wait()
    first_loads[1].wait()
    v = vectors_in[...]
    v = v / (1.0 + jnp.exp(-v))
    which = lax.broadcasted_iota(jnp.int32, (ROWS, depth), 0)
    vectors = jnp.where(
        which == 0,
        jnp.broadcast_to(v[0:1], (ROWS, depth)),
        jnp.broadcast_to(v[1:2], (ROWS, depth)),
    ).astype(jnp.bfloat16)
    first_loads[2].wait()
    for r in range(3):
        found = jnp.dot(vectors, mod_weight[r], preferred_element_type=jnp.float32)
        mod_parts[s, 2 * r : 2 * r + 2, :] = found[0:2]
    mod_parts[s, 6:8, :] = jnp.zeros((2, piece), jnp.float32)

    def part_copy(k, owner):
        return remote(
            mod_parts.at[owner],
            mod_parts.at[owner],
            part_send,
            part_recv.at[owner],
            sp=lax.rem(s + k, sp_size),
        )

    def piece_copy(k, owner):
        return remote(
            mod_pieces.at[owner],
            mod_pieces.at[owner],
            piece_send,
            piece_recv.at[owner],
            tp=lax.rem(t + 2 * k, tp_size),
        )

    def piece_across(owner):
        return remote(
            mod_pieces.at[owner],
            mod_pieces.at[owner],
            piece_send,
            piece_recv.at[owner],
            tp=twin,
        )

    def head_copy(core):
        return remote(per_head.at[core], per_head.at[core], head_sem.at[0], head_sem.at[1], tp=twin)

    def weight_copy(core):
        return remote(
            output_weight,
            weight.at[aligned(core * local, local, ROWS)],
            wo_sem.at[0],
            wo_sem.at[1],
            tp=twin,
        )

    for k in range(1, sp_size):
        part_copy(k, s).start()
    head_copy(c).start()
    for k in range(1, sp_size):
        part_copy(k, lax.rem(s + k, sp_size)).wait_recv()
    total = mod_parts[0]
    for i in range(1, sp_size):
        total = total + mod_parts[i]
    mod_pieces[t] = total
    for k in range(1, chips):
        piece_copy(k, t).start()
    piece_across(t).start()
    for part in range(half_parts, parts):
        send_mine(part)
    later_loads[-1].start()
    weight_copy(c).start()

    def forward(d, part):
        left = z - d
        right = z + d

        @pl.when(left >= 0)
        def _():
            token_copy(2, left, c, part).wait_recv()

            @pl.when(z + 1 < chips)
            def _():
                token_copy(0, left, c, part).start()

            token_copy(2, left, c, part).start()

        @pl.when(right < chips)
        def _():
            token_copy(2, right, c, part).wait_recv()

            @pl.when(z > 0)
            def _():
                token_copy(1, right, c, part).start()

            token_copy(2, right, c, part).start()

    for part in range(half_parts):
        forward(1, part)

    grid_rows = block_tokens // GRID_W
    all_rows = table.shape[1] - GRID_W
    later_loads[4].wait()
    is_row = lax.broadcasted_iota(jnp.int32, (GRID_W, half), 1) < half // 2
    for kind, into in enumerate((cosine, sine)):
        by_col = table[kind, all_rows:, :]
        for r in range(grid_rows):
            by_row = table[kind, pl.ds(s * grid_rows + r, 1), :]
            into[r * GRID_W : (r + 1) * GRID_W, :] = jnp.where(is_row, by_row, by_col)

    for k in range(1, chips):
        owner = lax.rem(t + 2 * k, tp_size)
        piece_copy(k, owner).wait_recv()
        piece_across(owner).start()
    for k in range(chips):
        piece_across(lax.rem(twin + 2 * k, tp_size)).wait_recv()
    for i in range(tp_size):
        found = mod_pieces[i]
        mod_rows[0:2, i * piece : (i + 1) * piece] = found[0:2]
        mod_rows[2:4, i * piece : (i + 1) * piece] = 1.0 + found[2:4]
        mod_rows[4:6, i * piece : (i + 1) * piece] = found[4:6]

    flip = jnp.where(2 * z >= chips, 0, 1)
    near = jnp.minimum(z, chips - 1 - z)
    far = jnp.maximum(z, chips - 1 - z)

    def block_of(i):
        r = jnp.maximum(i - (far - near), 0)
        single = i < far - near
        dist = jnp.where(single, far - i, near - lax.div(r, 2))
        turn_of = jnp.where(single, 0, lax.rem(r, 2))
        pick = turn_of + flip - 2 * turn_of * flip
        return z - dist + 2 * dist * pick

    def arrival(i):
        return block_of(chips - 1 - i)

    def swap(i):
        return jnp.where(i < 2, 1 - i, i) if chips > 2 else i

    tiles = width // LANES

    def normalise(ref, start, count, row):
        def group(g, carry):
            place = aligned(start(g), half_rows, ROWS)

            def tile(i):
                return ref[place, i * LANES : (i + 1) * LANES].astype(jnp.float32)

            sums = tile(0)
            for i in range(1, tiles):
                sums = sums + tile(i)
            center = jnp.sum(sums, axis=1, keepdims=True) * (1.0 / width)
            squares = jnp.zeros((half_rows, LANES), jnp.float32)
            for i in range(tiles):
                x = tile(i) - center
                squares = squares + x * x
            spread = jnp.sum(squares, axis=1, keepdims=True) * (1.0 / width)
            inverse = lax.rsqrt(spread + EPSILON)
            for i in range(tiles):
                cols = slice(i * LANES, (i + 1) * LANES)
                x = (tile(i) - center) * inverse
                y = x * mod_rows[2 + row : 3 + row, cols] + mod_rows[row : row + 1, cols]
                normed[aligned(g * half_rows, half_rows, ROWS), cols] = y.astype(jnp.bfloat16)
            return carry

        lax.fori_loop(0, count, group, 0)

    slots = chips + 2
    early = ctx_total + (chips - 1) * sp_size * pair

    def size_of(kind):
        return {"block": pair, "half": rows, "context": ctx_rows}[kind]

    def span_of(kind, slot):
        if kind == "context":
            return 0
        if kind == "block":
            return ctx_total + slot * sp_size * pair
        return early + (slot - (chips - 1)) * sp_size * rows

    def kv_place(kind, slot, owner):
        size = size_of(kind)
        return aligned(span_of(kind, slot) + owner * size, size, ROWS)

    def stage_place(kind, slot):
        if kind == "context":
            return pl.ds(block_tokens, ctx_rows)
        start = slot * pair if kind == "block" else (chips - 1) * pair + (slot - chips + 1) * rows
        return aligned(start, size_of(kind), ROWS)

    def kv_copy(k, owner, kind, slot):
        to = lax.rem(s + k, sp_size)
        return remote(
            kv_stage.at[lax.rem(to, heads), stage_place(kind, slot)],
            keys_values.at[kv_place(kind, slot, owner)],
            kv_send.at[k],
            kv_recv.at[owner, slot],
            sp=to,
        )

    def wanted(k):
        to = lax.rem(s + k, sp_size)
        return lax.div(lax.rem(to, plane), heads) == c

    def twin_copy(owner, kind, slot):
        place = keys_values.at[kv_place(kind, slot, owner)]
        return remote(place, place, kv_twin.at[0], kv_pass.at[slot], tp=twin)

    def twin_all(kind, slot):
        place = keys_values.at[
            aligned(span_of(kind, slot), sp_size * size_of(kind), ROWS)
        ]
        return remote(place, place, kv_twin.at[0], kv_pass.at[slot], tp=twin)

    def hand_out(keys, values, kind, slot):
        place = stage_place(kind, slot)
        for g in range(heads):
            kv_stage[g, place, :head] = keys[:, g * head : (g + 1) * head]
            kv_stage[g, place, head:] = values[:, g * head : (g + 1) * head]
        for k in range(1, sp_size):

            @pl.when(wanted(k))
            def _():
                kv_copy(k, s, kind, slot).start()

        @pl.when(is_owner)
        def _():
            keys_values[kv_place(kind, slot, s), :] = kv_stage[mine, place, :]
            twin_copy(s, kind, slot).start()

    def pass_on(kind, slot):
        @pl.when(is_owner)
        def _():
            for k in range(1, sp_size):
                owner = lax.rem(s + k, sp_size)
                kv_copy(k, owner, kind, slot).wait_recv()
                twin_copy(owner, kind, slot).start()

    def take(kind, slot):
        @pl.when(jnp.logical_not(is_owner))
        def _():
            twin_all(kind, slot).wait_recv()

    def q_copy(g, rel, source, b, start, count):
        core = c + rel - 2 * c * rel
        return remote(
            q_stage.at[g, aligned(b * pair + core * rows + start, count, ROWS)],
            queries.at[b, aligned(source * rows + start, count, ROWS)],
            q_send.at[2 * g + rel],
            q_recv.at[source, b],
            sp=base + c * heads + g,
            tp=twin if rel else t,
        )

    def out_copy(b, k, index):
        to = lax.rem(my_head + k, plane)
        return remote(
            out_stage.at[b, aligned(to * rows, rows, ROWS)],
            attended.at[b, index],
            out_send.at[k],
            out_recv.at[b, index],
            sp=base + to,
        )

    quarter = half // 4

    def turn(raw, cos, sin):
        lane = lax.broadcasted_iota(jnp.int32, cos.shape, 1)
        low = lax.rem(lane, 2 * quarter) < quarter
        found = []
        for i in range(local // half):
            v = raw[:, i * half : (i + 1) * half].astype(jnp.bfloat16).astype(jnp.float32)
            other = jnp.where(low, pltpu.roll(v, half - quarter, 1), pltpu.roll(v, quarter, 1))
            found.append((v * cos + other * sin).astype(jnp.bfloat16))
        return jnp.concatenate(found, axis=1)

    def process(b, kind, slot, start):
        count = rows if kind == "block" else half_rows
        first_part = start // ROWS
        for i in range(count // ROWS):
            token_copy(2, b, 1 - c, first_part + i).wait_recv()
        if kind == "block":
            normalise(tokens, lambda g: b * pair + g * half_rows, 4, 0)
        else:
            normalise(tokens, lambda g: b * pair + g * rows + start, 2, 0)

        def of(ref):
            if kind == "block":
                return ref[aligned(b * pair, pair, ROWS), :]
            return jnp.concatenate(
                [
                    ref[aligned(b * pair + core * rows + start, half_rows, ROWS), :]
                    for core in range(2)
                ],
                axis=0,
            )

        cos, sin = of(cosine), of(sine)
        x = normed[: 2 * count, :]
        hand_out(
            turn(jnp.dot(x, wk[...], preferred_element_type=jnp.float32), cos, sin),
            jnp.dot(x, wv[...], preferred_element_type=jnp.float32).astype(jnp.bfloat16),
            kind,
            slot,
        )
        turned = turn(jnp.dot(x, wq[...], preferred_element_type=jnp.float32), cos, sin)
        for g in range(heads):
            for core in range(2):
                q_stage[g, aligned(b * pair + core * rows + start, count, ROWS), :] = turned[
                    core * count : (core + 1) * count, g * head : (g + 1) * head
                ]
            q_copy(g, 1, my_head, b, start, count).start()

            @pl.when(c * heads + g != my_head)
            def _():
                q_copy(g, 0, my_head, b, start, count).start()

            @pl.when(c * heads + g == my_head)
            def _():
                queries[b, aligned(my_head * rows + start, count, ROWS), :] = q_stage[
                    g, aligned(b * pair + c * rows + start, count, ROWS), :
                ]

    for i in (1, 2, 3):
        later_loads[i].wait()
    normalise(context_tokens, lambda g: g * half_rows, ctx_rows // half_rows, 1)
    hand_out(
        jnp.dot(normed[:ctx_rows, :], wk[...], preferred_element_type=jnp.float32).astype(
            jnp.bfloat16
        ),
        jnp.dot(normed[:ctx_rows, :], wv[...], preferred_element_type=jnp.float32).astype(
            jnp.bfloat16
        ),
        "context",
        slots - 1,
    )
    for part in range(half_parts, parts):
        forward(1, part)
    later_loads[0].wait()
    later_loads[5].wait()

    def forwarded(i):
        dist = jnp.abs(arrival(i) - z)
        ahead = jnp.where(i == 1, half_parts, jnp.where(i == 2, parts - 1, parts))
        return jnp.where(near == 0, dist * parts, jnp.minimum(dist * parts + ahead, far * parts))

    def forward_all(start, stop):
        def one(q, carry):
            forward(1 + lax.div(q, parts), lax.rem(q, parts))
            return carry

        lax.fori_loop(start, stop, one, 0)

    def step(i, done):
        goal = jnp.where(i > 0, jnp.maximum(forwarded(i), done), done)
        forward_all(done, goal)
        process(arrival(i), "block", i, 0)

        @pl.when(i == 0)
        def _():
            pass_on("context", slots - 1)

        @pl.when(i > 0)
        def _():
            pass_on("block", i - 1)

        return goal

    done = lax.fori_loop(0, chips - 1, step, jnp.int32(parts))
    half_way = jnp.maximum(
        done, jnp.where(near == 0, (far - 1) * parts + half_parts, far * parts)
    )
    farthest = arrival(chips - 1)
    forward_all(done, half_way)
    process(farthest, "half", chips - 1, 0)
    pass_on("block", chips - 2)

    tile = plane * rows
    factor = half ** (-0.5) * LOG2E
    head_copy(1 - c).wait_recv()
    later_loads[6].wait()
    weight_of_second = per_head[owner_core, pl.ds(2 * mine, 1), :][:, 0:1]
    raised = per_head[owner_core, pl.ds(2 * mine + 1, 1), :][:, 0:1] * LOG2E

    def partial(b, m, start, stop, lifted):
        scores = (
            lax.dot_general(
                queries[b, :, m * half : (m + 1) * half],
                keys_values[start:stop, m * half : (m + 1) * half],
                (((1,), (1,)), ((), ())),
                preferred_element_type=jnp.float32,
            )
            * factor
        )
        if lifted:
            scores = jnp.concatenate([scores[:, :lifted] + raised, scores[:, lifted:]], axis=1)
        peak = jnp.max(scores, axis=1, keepdims=True)
        weights = jnp.exp2(scores - peak)
        sums = jnp.sum(weights, axis=1, keepdims=True)
        found = jnp.dot(
            weights.astype(jnp.bfloat16),
            keys_values[start:stop, head:],
            preferred_element_type=jnp.float32,
        )
        return peak, sums, found

    def wait_queries(b):
        for k in range(plane):
            source = lax.rem(my_head + k, plane)

            @pl.when(jnp.logical_or(k > 0, jnp.logical_not(is_owner)))
            def _():
                q_copy(0, 0, source, b, 0, rows).wait_recv()

    def begin(b):
        wait_queries(b)
        for m in range(2):
            peak, sums, found = partial(b, m, 0, early, ctx_total)
            held_peak[m] = jnp.broadcast_to(peak, (tile, LANES))
            held_sums[m] = jnp.broadcast_to(sums, (tile, LANES))
            held[m] = found

    def finish(b):
        outs = []
        for m in range(2):
            peak, sums, found = partial(b, m, early, keys_values.shape[0], 0)
            old_peak = held_peak[m][:, 0:1]
            top = jnp.maximum(peak, old_peak)
            now = jnp.exp2(peak - top)
            before = jnp.exp2(old_peak - top)
            sums = sums * now + held_sums[m][:, 0:1] * before
            outs.append((found * now + held[m] * before) / sums)
        hand_back(b, outs)

    def whole(b):
        wait_queries(b)
        outs = []
        for m in range(2):
            _, sums, found = partial(b, m, 0, keys_values.shape[0], ctx_total)
            outs.append(found / sums)
        hand_back(b, outs)

    def hand_back(b, outs):
        diff = outs[0] - weight_of_second * outs[1]
        mean = jnp.sum(diff * diff, axis=1, keepdims=True) * (1.0 / head)
        out_stage[b, :, :] = (diff * lax.rsqrt(mean + EPSILON) * gain[...]).astype(jnp.bfloat16)
        for k in range(1, plane):
            out_copy(b, k, my_head).start()
        attended[b, my_head] = out_stage[b, aligned(my_head * rows, rows, ROWS), :]

    forward_all(half_way, jnp.maximum(half_way, far * parts))
    process(farthest, "half", chips, half_rows)
    pass_on("half", chips - 1)
    take("context", slots - 1)

    def take_block(i, carry):
        take("block", i)
        return carry

    lax.fori_loop(0, chips - 1, take_block, 0)
    begin(block_of(swap(0)))
    pass_on("half", chips)
    take("half", chips - 1)
    take("half", chips)
    finish(block_of(swap(0)))
    weight_copy(1 - c).wait_recv()
    later_loads[7].wait()

    span = width // UNITS
    at_end = (z == 0) | (z + 1 == chips)

    def right_copy(u):
        return remote(stage.at[u], from_left.at[u], stage_sem.at[0], left_sem.at[u], tp=t + 2)

    def left_copy(u):
        return remote(stage.at[u], from_right.at[u], stage_sem.at[0], right_sem.at[u], tp=t - 2)

    def project(b):
        for k in range(1, plane):
            out_copy(b, k, lax.rem(my_head + k, plane)).wait_recv()
        x = jnp.concatenate([attended[b, g] for g in range(plane)], axis=1)
        for n in range(UNITS):
            u = b * UNITS + n
            found = jnp.dot(
                x, weight[:, n * span : (n + 1) * span], preferred_element_type=jnp.float32
            )
            own[u] = found

            @pl.when(at_end & (b != z))
            def _():
                stage[u] = found.astype(jnp.bfloat16)

                @pl.when(z == 0)
                def _():
                    right_copy(u).start()

                @pl.when(z > 0)
                def _():
                    left_copy(u).start()

    def attend_step(i, carry):
        @pl.when(i + 1 < chips)
        def _():
            whole(block_of(swap(i + 1)))

        project(block_of(swap(i)))
        return carry

    lax.fori_loop(0, chips, attend_step, 0)

    def copies_left():
        for k in range(1, plane):
            remote(
                attended.at[:, 0], attended.at[:, 0], out_send.at[k], out_recv.at[0, 0], tp=twin
            ).wait_send()

        def sent_tokens(b, carry):
            place = tokens.at[aligned(b * rows, rows, ROWS)]

            @pl.when((b <= z) & (z + 1 < chips))
            def _():
                remote(place, place, tok_send.at[0, b], tok_recv.at[0], tp=twin).wait_send()

            @pl.when((b >= z) & (z > 0))
            def _():
                remote(place, place, tok_send.at[1, b], tok_recv.at[0], tp=twin).wait_send()

            return carry

        lax.fori_loop(0, chips, sent_tokens, 0)
        place = tokens.at[: chips * rows]
        remote(place, place, tok_send.at[2, 0], tok_recv.at[0], tp=twin).wait_send()
        for g in range(heads):
            place = q_stage.at[g, : chips * rows]
            remote(place, place, q_send.at[2 * g + 1], q_recv.at[0, 0], tp=twin).wait_send()

            @pl.when(c * heads + g != my_head)
            def _():
                remote(place, place, q_send.at[2 * g], q_recv.at[0, 0], tp=twin).wait_send()

        for k in range(1, sp_size):

            @pl.when(wanted(k))
            def _():
                place = kv_stage.at[0]
                remote(place, place, kv_send.at[k], kv_recv.at[0, 0], tp=twin).wait_send()

        @pl.when(is_owner)
        def _():
            remote(
                keys_values, keys_values, kv_twin.at[0], kv_pass.at[0], tp=twin
            ).wait_send()

        place = mod_parts.at[: sp_size - 1]
        remote(place, place, part_send, part_recv.at[0], tp=twin).wait_send()
        place = mod_pieces.at[: tp_size - 1]
        remote(place, place, piece_send, piece_recv.at[0], tp=twin).wait_send()
        head_copy(c).wait_send()
        weight_copy(c).wait_send()

    copies_left()

    hop = 2

    def combine_step(i, carry):
        q = jnp.maximum(i - hop * (chips - 1 - z), 0)
        b = swap(lax.div(q, UNITS))
        u = b * UNITS + lax.rem(q, UNITS)

        @pl.when((i >= hop * (chips - 1 - z)) & (b < z))
        def _():
            left_copy(u).wait_recv()
            stage[u] = (own[u] + from_right[u].astype(jnp.float32)).astype(jnp.bfloat16)
            left_copy(u).start()

        p = jnp.maximum(i - hop * z, 0)
        e = chips - 1 - swap(lax.div(p, UNITS))
        v = e * UNITS + lax.rem(p, UNITS)

        @pl.when((i >= hop * z) & (e > z))
        def _():
            right_copy(v).wait_recv()
            stage[v] = (own[v] + from_left[v].astype(jnp.float32)).astype(jnp.bfloat16)
            right_copy(v).start()

        return carry

    @pl.when(jnp.logical_not(at_end))
    def _():
        lax.fori_loop(0, (chips - 1) * UNITS + hop * (chips - 1), combine_step, 0)

    for n in range(UNITS):
        u = z * UNITS + n
        cols = slice(n * span, (n + 1) * span)

        @pl.when(z > 0)
        def _():
            right_copy(u).wait_recv()
            own[u] = own[u] + from_left[u].astype(jnp.float32)

        @pl.when(z + 1 < chips)
        def _():
            left_copy(u).wait_recv()
            own[u] = own[u] + from_right[u].astype(jnp.float32)

        result[:, cols] = (
            tokens[aligned(t * rows, rows, ROWS), cols].astype(jnp.float32)
            + mod_rows[4:5, cols] * own[u]
        ).astype(jnp.bfloat16)

    place = stage.at[: (chips - 1) * UNITS]
    remote(place, place, stage_sem.at[0], left_sem.at[0], tp=twin).wait_send()


def tables(grid_rows, half):
    quarter = half // 4
    inverse = (ROPE_BASE ** (-np.arange(quarter) / quarter)).astype(np.float32)
    sign = np.where(np.arange(half) % (2 * quarter) < quarter, -1.0, 1.0)
    places = np.concatenate([np.arange(grid_rows), np.arange(GRID_W)]).astype(np.float32)
    angles = (places[:, None] * np.tile(inverse, 4)).astype(np.float64)
    return np.stack([np.cos(angles), np.sin(angles) * sign]).astype(np.float32)


def shards(
    sp_size,
    tp_size,
    latent,
    context,
    condition,
    context_condition,
    modulation,
    query_weight,
    key_weight,
    value_weight,
    lambdas,
    context_lift,
    head_gain,
    output_weight,
):
    rows, width = latent.shape
    chips = tp_size // 2
    local = query_weight.shape[1]
    heads = lambdas.shape[0]
    head = local // heads
    half = head // 2
    plane = 2 * heads
    block_tokens = rows * tp_size
    ctx_rows = context.shape[0]
    piece = modulation.shape[2]
    depth = modulation.shape[1]
    parts = rows // ROWS
    table = tables(sp_size * block_tokens // GRID_W, half)
    vmem = pl.BlockSpec(memory_space=pltpu.VMEM)
    smem = pl.BlockSpec(memory_space=pltpu.SMEM)
    anywhere = pl.BlockSpec(memory_space=pl.ANY)
    bf16, f32 = jnp.bfloat16, jnp.float32
    dma = pltpu.SemaphoreType.DMA
    units = (UNITS * chips, rows, width // UNITS)
    return pl.pallas_call(
        functools.partial(block_kernel, sp_size, tp_size),
        out_shape=jax.ShapeDtypeStruct((rows, width), bf16),
        in_specs=[anywhere] * 9 + [smem] * 2 + [anywhere] * 2,
        out_specs=vmem,
        scratch_shapes=[
            pltpu.VMEM((block_tokens, width), bf16),
            pltpu.VMEM(context.shape, bf16),
            pltpu.VMEM((max(2 * rows, ctx_rows), width), bf16),
            pltpu.VMEM(modulation.shape, bf16),
            pltpu.VMEM((width, local), bf16),
            pltpu.VMEM((width, local), bf16),
            pltpu.VMEM((width, local), bf16),
            pltpu.VMEM((2 * local, width), bf16),
            pltpu.VMEM((sp_size * (ctx_rows + block_tokens), 2 * head), bf16),
            pltpu.VMEM((chips, plane * rows, head), bf16),
            pltpu.VMEM((heads, block_tokens + ctx_rows, 2 * head), bf16),
            pltpu.VMEM((heads, block_tokens, head), bf16),
            pltpu.VMEM((chips, plane * rows, head), bf16),
            pltpu.VMEM((chips, plane, rows, head), bf16),
            pltpu.VMEM(units, f32),
            pltpu.VMEM(units, bf16),
            pltpu.VMEM(units, bf16),
            pltpu.VMEM(units, bf16),
            pltpu.VMEM((sp_size, 8, piece), f32),
            pltpu.VMEM((tp_size, 8, piece), f32),
            pltpu.VMEM((8, width), f32),
            pltpu.VMEM((2, depth), f32),
            pltpu.VMEM(table.shape, f32),
            pltpu.VMEM((block_tokens, half), f32),
            pltpu.VMEM((block_tokens, half), f32),
            pltpu.VMEM((1, head), f32),
            pltpu.VMEM((2, 8, LANES), f32),
            pltpu.VMEM((2, plane * rows, head), f32),
            pltpu.VMEM((2, plane * rows, LANES), f32),
            pltpu.VMEM((2, plane * rows, LANES), f32),
            dma((11,)),
            dma((3, chips)),
            dma((parts * tp_size,)),
            dma(()),
            dma((sp_size,)),
            dma(()),
            dma((tp_size,)),
            dma((sp_size,)),
            dma((1,)),
            dma((sp_size, chips + 2)),
            dma((chips + 2,)),
            dma((2 * heads,)),
            dma((plane, chips)),
            dma((plane,)),
            dma((chips, plane)),
            dma((2,)),
            dma((2,)),
            dma((1,)),
            dma((UNITS * chips,)),
            dma((UNITS * chips,)),
        ],
        compiler_params=pltpu.CompilerParams(
            collective_id=0, has_side_effects=True, vmem_limit_bytes=VMEM_LIMIT
        ),
        name="block",
    )(
        latent,
        context,
        condition.reshape(1, -1),
        context_condition.reshape(1, -1),
        modulation,
        query_weight,
        key_weight,
        value_weight,
        table,
        lambdas,
        context_lift,
        head_gain.reshape(1, -1),
        output_weight,
    )


def solution(mesh):
    in_specs = (
        P(("sp", "tp"), None),
        P("sp", None),
        P(),
        P(),
        P(None, "sp", "tp"),
        P(None, "tp"),
        P(None, "tp"),
        P(None, "tp"),
        P("tp"),
        P("tp"),
        P(),
        P("tp", None),
    )
    out_specs = P(("sp", "tp"), None)
    body = functools.partial(shards, mesh.shape["sp"], mesh.shape["tp"])
    return jax.shard_map(body, mesh=mesh, in_specs=in_specs, out_specs=out_specs, check_vma=False)
```

```python
import functools

import jax
import jax.numpy as jnp
import numpy as np
from jax import lax
from jax.experimental import pallas as pl
from jax.experimental.pallas import tpu as pltpu
from jax.sharding import PartitionSpec as P

GRID_W = 64
ROPE_BASE = 10000.0
EPSILON = 1e-05
LOG2E = 1.4426950408889634
ROWS = 16
LANES = 128
UNITS = 4
VMEM_LIMIT = 53 * 1024 * 1024
MESH = pl.DeviceIdType.MESH


def remote(src, dst, send_sem, recv_sem, **where):
    return pltpu.make_async_remote_copy(
        src_ref=src,
        dst_ref=dst,
        send_sem=send_sem,
        recv_sem=recv_sem,
        device_id=where,
        device_id_type=MESH,
    )


def aligned(start, size, unit):
    return pl.ds(pl.multiple_of(start, unit), size)


def block_kernel(
    sp_size,
    tp_size,
    latent,
    context,
    condition,
    context_condition,
    modulation,
    query_weight,
    key_weight,
    value_weight,
    tables,
    lambdas,
    lift,
    gain_in,
    output_weight,
    result,
    tokens,
    context_tokens,
    normed,
    mod_weight,
    wq,
    wk,
    wv,
    weight,
    keys_values,
    queries,
    kv_stage,
    q_stage,
    out_stage,
    attended,
    own,
    stage,
    from_left,
    from_right,
    mod_parts,
    mod_pieces,
    mod_rows,
    vectors_in,
    table,
    cosine,
    sine,
    gain,
    per_head,
    scalars,
    held,
    held_peak,
    held_sums,
    local_sem,
    tok_send,
    tok_recv,
    part_send,
    part_recv,
    piece_send,
    piece_recv,
    kv_send,
    kv_twin,
    kv_recv,
    kv_pass,
    q_send,
    q_recv,
    out_send,
    out_recv,
    wo_sem,
    head_sem,
    stage_sem,
    left_sem,
    right_sem,
):
    s = lax.axis_index("sp")
    t = lax.axis_index("tp")
    z = lax.div(t, 2)
    c = lax.rem(t, 2)
    twin = t + 1 - 2 * c
    chips = tp_size // 2
    rows, width = latent.shape
    parts = rows // ROWS
    half_rows = rows // 2
    half_parts = parts // 2
    pair = 2 * rows
    block_tokens = tp_size * rows
    ctx_rows = context.shape[0]
    ctx_total = ctx_rows * sp_size
    local = query_weight.shape[1]
    head = gain_in.shape[1]
    heads = local // head
    half = head // 2
    plane = 2 * heads
    piece = modulation.shape[2]
    depth = modulation.shape[1]
    my_head = lax.rem(s, plane)
    base = s - my_head
    owner_core = lax.div(my_head, heads)
    mine = lax.rem(my_head, heads)
    is_owner = c == owner_core
    ctx_item = 2 * chips

    def load(i, src, dst):
        return pltpu.make_async_copy(src, dst, local_sem.at[i])

    own_slot = tokens.at[aligned(t * rows, rows, ROWS)]
    local_rows = aligned(c * local, local, ROWS)
    here = aligned(s * depth, depth, LANES)
    first_loads = [
        load(0, condition.at[:, here], vectors_in.at[0:1]),
        load(1, context_condition.at[:, here], vectors_in.at[1:2]),
        load(2, modulation, mod_weight),
        load(11, lambdas, scalars.at[0]),
        load(12, lift, scalars.at[1]),
    ]
    later_loads = [
        load(3, latent, own_slot),
        load(4, context, context_tokens),
        load(5, key_weight, wk),
        load(6, value_weight, wv),
        load(7, tables, table),
        load(8, query_weight, wq),
        load(9, gain_in, gain),
        load(10, output_weight, weight.at[local_rows]),
    ]
    barrier = pltpu.get_barrier_semaphore()
    for k in range(1, tp_size):
        pl.semaphore_signal(
            barrier, inc=1, device_id={"tp": lax.rem(t + k, tp_size)}, device_id_type=MESH
        )
    for k in range(1, sp_size):
        for to in (t, twin):
            pl.semaphore_signal(
                barrier,
                inc=1,
                device_id={"sp": lax.rem(s + k, sp_size), "tp": to},
                device_id_type=MESH,
            )
    for copy in first_loads + later_loads[:-1]:
        copy.start()
    pl.semaphore_wait(barrier, tp_size - 1 + 2 * (sp_size - 1))

    def token_copy(kind, b, core, part, mine_first=False):
        slot = 2 * b + core
        place = tokens.at[aligned(slot * rows + part * ROWS, ROWS, ROWS)]
        to = (t + 2, t - 2, twin)[kind]
        return remote(
            latent.at[aligned(part * ROWS, ROWS, ROWS)] if mine_first else place,
            place,
            tok_send.at[kind, 0 if kind == 2 else b],
            tok_recv.at[parts * slot + part],
            tp=to,
        )

    def send_mine(part):
        @pl.when(z + 1 < chips)
        def _():
            token_copy(0, z, c, part, True).start()

        @pl.when(z > 0)
        def _():
            token_copy(1, z, c, part, True).start()

        token_copy(2, z, c, part, True).start()

    for part in range(half_parts):
        send_mine(part)

    first_loads[0].wait()
    first_loads[1].wait()
    v = vectors_in[...]
    v = v / (1.0 + jnp.exp(-v))
    which = lax.broadcasted_iota(jnp.int32, (ROWS, depth), 0)
    vectors = jnp.where(
        which == 0,
        jnp.broadcast_to(v[0:1], (ROWS, depth)),
        jnp.broadcast_to(v[1:2], (ROWS, depth)),
    ).astype(jnp.bfloat16)
    first_loads[3].wait()
    first_loads[4].wait()
    for i in range(2):
        for g in range(heads):
            per_head[c, 2 * g + i : 2 * g + i + 1, :] = jnp.broadcast_to(
                scalars[i][:, g : g + 1], (1, LANES)
            )
    first_loads[2].wait()
    for r in range(3):
        found = jnp.dot(vectors, mod_weight[r], preferred_element_type=jnp.float32)
        mod_parts[s, 2 * r : 2 * r + 2, :] = found[0:2]
    mod_parts[s, 6:8, :] = jnp.zeros((2, piece), jnp.float32)

    def part_copy(k, owner):
        return remote(
            mod_parts.at[owner],
            mod_parts.at[owner],
            part_send,
            part_recv.at[owner],
            sp=lax.rem(s + k, sp_size),
        )

    def piece_copy(k, owner):
        return remote(
            mod_pieces.at[owner],
            mod_pieces.at[owner],
            piece_send,
            piece_recv.at[owner],
            tp=lax.rem(t + 2 * k, tp_size),
        )

    def piece_across(owner):
        return remote(
            mod_pieces.at[owner],
            mod_pieces.at[owner],
            piece_send,
            piece_recv.at[owner],
            tp=twin,
        )

    def head_copy(core):
        return remote(per_head.at[core], per_head.at[core], head_sem.at[0], head_sem.at[1], tp=twin)

    def weight_copy(core):
        return remote(
            output_weight,
            weight.at[aligned(core * local, local, ROWS)],
            wo_sem.at[0],
            wo_sem.at[1],
            tp=twin,
        )

    for k in range(1, sp_size):
        part_copy(k, s).start()
    head_copy(c).start()
    for k in range(1, sp_size):
        part_copy(k, lax.rem(s + k, sp_size)).wait_recv()
    total = mod_parts[0]
    for i in range(1, sp_size):
        total = total + mod_parts[i]
    mod_pieces[t] = total
    for k in range(1, chips):
        piece_copy(k, t).start()
    piece_across(t).start()
    for part in range(half_parts, parts):
        send_mine(part)
    later_loads[-1].start()
    weight_copy(c).start()

    def forward(d, part):
        left = z - d
        right = z + d

        @pl.when(left >= 0)
        def _():
            token_copy(2, left, c, part).wait_recv()

            @pl.when(z + 1 < chips)
            def _():
                token_copy(0, left, c, part).start()

            token_copy(2, left, c, part).start()

        @pl.when(right < chips)
        def _():
            token_copy(2, right, c, part).wait_recv()

            @pl.when(z > 0)
            def _():
                token_copy(1, right, c, part).start()

            token_copy(2, right, c, part).start()

    for part in range(half_parts):
        forward(1, part)

    grid_rows = block_tokens // GRID_W
    all_rows = table.shape[1] - GRID_W
    later_loads[4].wait()
    is_row = lax.broadcasted_iota(jnp.int32, (GRID_W, half), 1) < half // 2
    for kind, into in enumerate((cosine, sine)):
        by_col = table[kind, all_rows:, :]
        for r in range(grid_rows):
            by_row = table[kind, pl.ds(s * grid_rows + r, 1), :]
            into[r * GRID_W : (r + 1) * GRID_W, :] = jnp.where(is_row, by_row, by_col)

    for k in range(1, chips):
        owner = lax.rem(t + 2 * k, tp_size)
        piece_copy(k, owner).wait_recv()
        piece_across(owner).start()
    for k in range(chips):
        piece_across(lax.rem(twin + 2 * k, tp_size)).wait_recv()
    for i in range(tp_size):
        found = mod_pieces[i]
        mod_rows[0:2, i * piece : (i + 1) * piece] = found[0:2]
        mod_rows[2:4, i * piece : (i + 1) * piece] = 1.0 + found[2:4]
        mod_rows[4:6, i * piece : (i + 1) * piece] = found[4:6]

    flip = jnp.where(2 * z >= chips, 0, 1)
    near = jnp.minimum(z, chips - 1 - z)
    far = jnp.maximum(z, chips - 1 - z)

    def block_of(i):
        r = jnp.maximum(i - (far - near), 0)
        single = i < far - near
        dist = jnp.where(single, far - i, near - lax.div(r, 2))
        turn_of = jnp.where(single, 0, lax.rem(r, 2))
        pick = turn_of + flip - 2 * turn_of * flip
        return z - dist + 2 * dist * pick

    def arrival(i):
        return block_of(chips - 1 - i)

    def swap(i):
        return jnp.where(i < 2, 1 - i, i) if chips > 2 else i

    tiles = width // LANES

    def normalise(ref, start, count, row):
        def group(g, carry):
            place = aligned(start(g), half_rows, ROWS)

            def tile(i):
                return ref[place, i * LANES : (i + 1) * LANES].astype(jnp.float32)

            sums = tile(0)
            for i in range(1, tiles):
                sums = sums + tile(i)
            center = jnp.sum(sums, axis=1, keepdims=True) * (1.0 / width)
            squares = jnp.zeros((half_rows, LANES), jnp.float32)
            for i in range(tiles):
                x = tile(i) - center
                squares = squares + x * x
            spread = jnp.sum(squares, axis=1, keepdims=True) * (1.0 / width)
            inverse = lax.rsqrt(spread + EPSILON)
            for i in range(tiles):
                cols = slice(i * LANES, (i + 1) * LANES)
                x = (tile(i) - center) * inverse
                y = x * mod_rows[2 + row : 3 + row, cols] + mod_rows[row : row + 1, cols]
                normed[aligned(g * half_rows, half_rows, ROWS), cols] = y.astype(jnp.bfloat16)
            return carry

        lax.fori_loop(0, count, group, 0)

    slots = chips + 2
    early = ctx_total + (chips - 1) * sp_size * pair
    most = early + sp_size * rows

    def size_of(kind):
        return {"block": pair, "half": rows, "context": ctx_rows}[kind]

    def span_of(kind, slot):
        if kind == "context":
            return 0
        if kind == "block":
            return ctx_total + slot * sp_size * pair
        return early + (slot - (chips - 1)) * sp_size * rows

    def kv_place(kind, slot, owner):
        size = size_of(kind)
        return aligned(span_of(kind, slot) + owner * size, size, ROWS)

    def stage_place(kind, slot):
        if kind == "context":
            return pl.ds(block_tokens, ctx_rows)
        start = slot * pair if kind == "block" else (chips - 1) * pair + (slot - chips + 1) * rows
        return aligned(start, size_of(kind), ROWS)

    def kv_copy(k, owner, kind, slot):
        to = lax.rem(s + k, sp_size)
        return remote(
            kv_stage.at[lax.rem(to, heads), stage_place(kind, slot)],
            keys_values.at[kv_place(kind, slot, owner)],
            kv_send.at[k],
            kv_recv.at[owner, slot],
            sp=to,
        )

    def wanted(k):
        to = lax.rem(s + k, sp_size)
        return lax.div(lax.rem(to, plane), heads) == c

    def twin_copy(owner, kind, slot):
        place = keys_values.at[kv_place(kind, slot, owner)]
        return remote(place, place, kv_twin.at[0], kv_pass.at[slot], tp=twin)

    def twin_all(kind, slot):
        place = keys_values.at[
            aligned(span_of(kind, slot), sp_size * size_of(kind), ROWS)
        ]
        return remote(place, place, kv_twin.at[0], kv_pass.at[slot], tp=twin)

    def hand_out(keys, values, kind, slot):
        place = stage_place(kind, slot)
        for g in range(heads):
            kv_stage[g, place, :head] = keys[:, g * head : (g + 1) * head]
            kv_stage[g, place, head:] = values[:, g * head : (g + 1) * head]
        for k in range(1, sp_size):

            @pl.when(wanted(k))
            def _():
                kv_copy(k, s, kind, slot).start()

        @pl.when(is_owner)
        def _():
            keys_values[kv_place(kind, slot, s), :] = kv_stage[mine, place, :]
            twin_copy(s, kind, slot).start()

    def pass_on(kind, slot):
        @pl.when(is_owner)
        def _():
            for k in range(1, sp_size):
                owner = lax.rem(s + k, sp_size)
                kv_copy(k, owner, kind, slot).wait_recv()
                twin_copy(owner, kind, slot).start()

    def take(kind, slot):
        @pl.when(jnp.logical_not(is_owner))
        def _():
            twin_all(kind, slot).wait_recv()

    def q_copy(g, rel, source, b, start, count):
        core = c + rel - 2 * c * rel
        return remote(
            q_stage.at[g, aligned(b * pair + core * rows + start, count, ROWS)],
            queries.at[b, aligned(source * rows + start, count, ROWS)],
            q_send.at[2 * g + rel],
            q_recv.at[source, b],
            sp=base + c * heads + g,
            tp=twin if rel else t,
        )

    def out_copy(b, k, index):
        to = lax.rem(my_head + k, plane)
        return remote(
            out_stage.at[b, aligned(to * rows, rows, ROWS)],
            attended.at[b, index],
            out_send.at[k],
            out_recv.at[b, index],
            sp=base + to,
        )

    quarter = half // 4

    def turn(raw, cos, sin):
        lane = lax.broadcasted_iota(jnp.int32, cos.shape, 1)
        low = lax.rem(lane, 2 * quarter) < quarter
        found = []
        for i in range(local // half):
            v = raw[:, i * half : (i + 1) * half].astype(jnp.bfloat16).astype(jnp.float32)
            other = jnp.where(low, pltpu.roll(v, half - quarter, 1), pltpu.roll(v, quarter, 1))
            found.append((v * cos + other * sin).astype(jnp.bfloat16))
        return jnp.concatenate(found, axis=1)

    def process(b, kind, slot, start):
        count = rows if kind == "block" else half_rows
        first_part = start // ROWS
        for i in range(count // ROWS):
            token_copy(2, b, 1 - c, first_part + i).wait_recv()
        if kind == "block":
            normalise(tokens, lambda g: b * pair + g * half_rows, 4, 0)
        else:
            normalise(tokens, lambda g: b * pair + g * rows + start, 2, 0)

        def of(ref):
            if kind == "block":
                return ref[aligned(b * pair, pair, ROWS), :]
            return jnp.concatenate(
                [
                    ref[aligned(b * pair + core * rows + start, half_rows, ROWS), :]
                    for core in range(2)
                ],
                axis=0,
            )

        cos, sin = of(cosine), of(sine)
        x = normed[: 2 * count, :]
        hand_out(
            turn(jnp.dot(x, wk[...], preferred_element_type=jnp.float32), cos, sin),
            jnp.dot(x, wv[...], preferred_element_type=jnp.float32).astype(jnp.bfloat16),
            kind,
            slot,
        )
        turned = turn(jnp.dot(x, wq[...], preferred_element_type=jnp.float32), cos, sin)
        for g in range(heads):
            for core in range(2):
                q_stage[g, aligned(b * pair + core * rows + start, count, ROWS), :] = turned[
                    core * count : (core + 1) * count, g * head : (g + 1) * head
                ]
            q_copy(g, 1, my_head, b, start, count).start()

            @pl.when(c * heads + g != my_head)
            def _():
                q_copy(g, 0, my_head, b, start, count).start()

            @pl.when(c * heads + g == my_head)
            def _():
                queries[b, aligned(my_head * rows + start, count, ROWS), :] = q_stage[
                    g, aligned(b * pair + c * rows + start, count, ROWS), :
                ]

    for i in (1, 2, 3):
        later_loads[i].wait()
    normalise(context_tokens, lambda g: g * half_rows, ctx_rows // half_rows, 1)
    hand_out(
        jnp.dot(normed[:ctx_rows, :], wk[...], preferred_element_type=jnp.float32).astype(
            jnp.bfloat16
        ),
        jnp.dot(normed[:ctx_rows, :], wv[...], preferred_element_type=jnp.float32).astype(
            jnp.bfloat16
        ),
        "context",
        slots - 1,
    )
    for part in range(half_parts, parts):
        forward(1, part)
    later_loads[0].wait()
    later_loads[5].wait()

    def forwarded(i):
        dist = jnp.abs(arrival(i) - z)
        ahead = jnp.where(i == 1, half_parts, jnp.where(i == 2, parts - 1, parts))
        return jnp.where(near == 0, dist * parts, jnp.minimum(dist * parts + ahead, far * parts))

    def forward_all(start, stop):
        def one(q, carry):
            forward(1 + lax.div(q, parts), lax.rem(q, parts))
            return carry

        lax.fori_loop(start, stop, one, 0)

    def step(i, done):
        goal = jnp.where(i > 0, jnp.maximum(forwarded(i), done), done)
        forward_all(done, goal)
        process(arrival(i), "block", i, 0)

        @pl.when(i == 0)
        def _():
            pass_on("context", slots - 1)

        @pl.when(i > 0)
        def _():
            pass_on("block", i - 1)

        return goal

    done = lax.fori_loop(0, chips - 1, step, jnp.int32(parts))
    half_way = jnp.maximum(
        done, jnp.where(near == 0, (far - 1) * parts + half_parts, far * parts)
    )
    farthest = arrival(chips - 1)
    forward_all(done, half_way)
    process(farthest, "half", chips - 1, 0)
    pass_on("block", chips - 2)

    tile = plane * rows
    factor = half ** (-0.5) * LOG2E
    head_copy(1 - c).wait_recv()
    later_loads[6].wait()
    weight_of_second = per_head[owner_core, pl.ds(2 * mine, 1), :][:, 0:1]
    raised = per_head[owner_core, pl.ds(2 * mine + 1, 1), :][:, 0:1] * LOG2E

    def partial(b, m, start, stop, lifted):
        scores = (
            lax.dot_general(
                queries[b, :, m * half : (m + 1) * half],
                keys_values[start:stop, m * half : (m + 1) * half],
                (((1,), (1,)), ((), ())),
                preferred_element_type=jnp.float32,
            )
            * factor
        )
        if lifted:
            scores = jnp.concatenate([scores[:, :lifted] + raised, scores[:, lifted:]], axis=1)
        peak = jnp.max(scores, axis=1, keepdims=True)
        weights = jnp.exp2(scores - peak)
        sums = jnp.sum(weights, axis=1, keepdims=True)
        found = jnp.dot(
            weights.astype(jnp.bfloat16),
            keys_values[start:stop, head:],
            preferred_element_type=jnp.float32,
        )
        return peak, sums, found

    def wait_queries(b):
        for k in range(plane):
            source = lax.rem(my_head + k, plane)

            @pl.when(jnp.logical_or(k > 0, jnp.logical_not(is_owner)))
            def _():
                q_copy(0, 0, source, b, 0, rows).wait_recv()

    def begin(b):
        wait_queries(b)
        for m in range(2):
            peak, sums, found = partial(b, m, 0, most, ctx_total)
            held_peak[m] = jnp.broadcast_to(peak, (tile, LANES))
            held_sums[m] = jnp.broadcast_to(sums, (tile, LANES))
            held[m] = found

    def finish(b):
        outs = []
        for m in range(2):
            peak, sums, found = partial(b, m, most, keys_values.shape[0], 0)
            old_peak = held_peak[m][:, 0:1]
            top = jnp.maximum(peak, old_peak)
            now = jnp.exp2(peak - top)
            before = jnp.exp2(old_peak - top)
            sums = sums * now + held_sums[m][:, 0:1] * before
            outs.append((found * now + held[m] * before) / sums)
        hand_back(b, outs)

    def whole(b):
        wait_queries(b)
        outs = []
        for m in range(2):
            _, sums, found = partial(b, m, 0, keys_values.shape[0], ctx_total)
            outs.append(found / sums)
        hand_back(b, outs)

    def hand_back(b, outs):
        diff = outs[0] - weight_of_second * outs[1]
        mean = jnp.sum(diff * diff, axis=1, keepdims=True) * (1.0 / head)
        out_stage[b, :, :] = (diff * lax.rsqrt(mean + EPSILON) * gain[...]).astype(jnp.bfloat16)
        for k in range(1, plane):
            out_copy(b, k, my_head).start()
        attended[b, my_head] = out_stage[b, aligned(my_head * rows, rows, ROWS), :]

    forward_all(half_way, jnp.maximum(half_way, far * parts))
    process(farthest, "half", chips, half_rows)
    pass_on("half", chips - 1)
    take("context", slots - 1)

    def take_block(i, carry):
        take("block", i)
        return carry

    lax.fori_loop(0, chips - 1, take_block, 0)
    take("half", chips - 1)
    begin(block_of(swap(0)))
    pass_on("half", chips)
    take("half", chips)
    finish(block_of(swap(0)))
    weight_copy(1 - c).wait_recv()
    later_loads[7].wait()

    span = width // UNITS
    at_end = (z == 0) | (z + 1 == chips)

    def right_copy(u):
        return remote(stage.at[u], from_left.at[u], stage_sem.at[0], left_sem.at[u], tp=t + 2)

    def left_copy(u):
        return remote(stage.at[u], from_right.at[u], stage_sem.at[0], right_sem.at[u], tp=t - 2)

    def project(b):
        for k in range(1, plane):
            out_copy(b, k, lax.rem(my_head + k, plane)).wait_recv()
        x = jnp.concatenate([attended[b, g] for g in range(plane)], axis=1)
        for n in range(UNITS):
            u = b * UNITS + n
            found = jnp.dot(
                x, weight[:, n * span : (n + 1) * span], preferred_element_type=jnp.float32
            )
            own[u] = found

            @pl.when(at_end & (b != z))
            def _():
                stage[u] = found.astype(jnp.bfloat16)

                @pl.when(z == 0)
                def _():
                    right_copy(u).start()

                @pl.when(z > 0)
                def _():
                    left_copy(u).start()

    hop = 2

    def combine_step(i, carry):
        q = jnp.maximum(i - hop * (chips - 1 - z), 0)
        b = swap(lax.div(q, UNITS))
        u = b * UNITS + lax.rem(q, UNITS)

        @pl.when((i >= hop * (chips - 1 - z)) & (b < z))
        def _():
            left_copy(u).wait_recv()
            stage[u] = (own[u] + from_right[u].astype(jnp.float32)).astype(jnp.bfloat16)
            left_copy(u).start()

        p = jnp.maximum(i - hop * z, 0)
        e = chips - 1 - swap(lax.div(p, UNITS))
        v = e * UNITS + lax.rem(p, UNITS)

        @pl.when((i >= hop * z) & (e > z))
        def _():
            right_copy(v).wait_recv()
            stage[v] = (own[v] + from_left[v].astype(jnp.float32)).astype(jnp.bfloat16)
            right_copy(v).start()

        return carry

    def combine(start, stop):
        @pl.when(jnp.logical_not(at_end))
        def _():
            lax.fori_loop(start, stop, combine_step, 0)

    steps = 2 * chips - 1

    def attend_step(k, carry):
        index = lax.div(k, 2)
        odd = lax.rem(k, 2) == 1
        attends = jnp.where(at_end, odd, jnp.logical_not(odd) & (k + 1 < steps))

        @pl.when(attends)
        def _():
            whole(block_of(swap(index + 1)))

        @pl.when(jnp.logical_not(attends))
        def _():
            project(block_of(swap(index)))

        @pl.when(k == steps - 3)
        def _():
            combine(0, hop + 1)

        @pl.when(k == steps - 2)
        def _():
            combine(hop + 1, hop + 2)

        return carry

    lax.fori_loop(0, steps, attend_step, 0)

    def copies_left():
        for k in range(1, plane):
            remote(
                attended.at[:, 0], attended.at[:, 0], out_send.at[k], out_recv.at[0, 0], tp=twin
            ).wait_send()

        def sent_tokens(b, carry):
            place = tokens.at[aligned(b * rows, rows, ROWS)]

            @pl.when((b <= z) & (z + 1 < chips))
            def _():
                remote(place, place, tok_send.at[0, b], tok_recv.at[0], tp=twin).wait_send()

            @pl.when((b >= z) & (z > 0))
            def _():
                remote(place, place, tok_send.at[1, b], tok_recv.at[0], tp=twin).wait_send()

            return carry

        lax.fori_loop(0, chips, sent_tokens, 0)
        place = tokens.at[: chips * rows]
        remote(place, place, tok_send.at[2, 0], tok_recv.at[0], tp=twin).wait_send()
        for g in range(heads):
            place = q_stage.at[g, : chips * rows]
            remote(place, place, q_send.at[2 * g + 1], q_recv.at[0, 0], tp=twin).wait_send()

            @pl.when(c * heads + g != my_head)
            def _():
                remote(place, place, q_send.at[2 * g], q_recv.at[0, 0], tp=twin).wait_send()

        for k in range(1, sp_size):

            @pl.when(wanted(k))
            def _():
                place = kv_stage.at[0]
                remote(place, place, kv_send.at[k], kv_recv.at[0, 0], tp=twin).wait_send()

        @pl.when(is_owner)
        def _():
            remote(
                keys_values, keys_values, kv_twin.at[0], kv_pass.at[0], tp=twin
            ).wait_send()

        place = mod_parts.at[: sp_size - 1]
        remote(place, place, part_send, part_recv.at[0], tp=twin).wait_send()
        place = mod_pieces.at[: tp_size - 1]
        remote(place, place, piece_send, piece_recv.at[0], tp=twin).wait_send()
        head_copy(c).wait_send()
        weight_copy(c).wait_send()

    copies_left()
    combine(hop + 2, (chips - 1) * (UNITS + hop))

    for n in range(UNITS):
        u = z * UNITS + n
        cols = slice(n * span, (n + 1) * span)

        @pl.when(z > 0)
        def _():
            right_copy(u).wait_recv()
            own[u] = own[u] + from_left[u].astype(jnp.float32)

        @pl.when(z + 1 < chips)
        def _():
            left_copy(u).wait_recv()
            own[u] = own[u] + from_right[u].astype(jnp.float32)

        result[:, cols] = (
            tokens[aligned(t * rows, rows, ROWS), cols].astype(jnp.float32)
            + mod_rows[4:5, cols] * own[u]
        ).astype(jnp.bfloat16)

    place = stage.at[: (chips - 1) * UNITS]
    remote(place, place, stage_sem.at[0], left_sem.at[0], tp=twin).wait_send()


def tables(grid_rows, half):
    quarter = half // 4
    inverse = (ROPE_BASE ** (-np.arange(quarter) / quarter)).astype(np.float32)
    sign = np.where(np.arange(half) % (2 * quarter) < quarter, -1.0, 1.0)
    places = np.concatenate([np.arange(grid_rows), np.arange(GRID_W)]).astype(np.float32)
    angles = (places[:, None] * np.tile(inverse, 4)).astype(np.float64)
    return np.stack([np.cos(angles), np.sin(angles) * sign]).astype(np.float32)


def row(x):
    return x.reshape(1, -1) if x.size > 1 else jnp.broadcast_to(x.reshape(1, 1), (1, LANES))


def shards(
    sp_size,
    tp_size,
    latent,
    context,
    condition,
    context_condition,
    modulation,
    query_weight,
    key_weight,
    value_weight,
    lambdas,
    context_lift,
    head_gain,
    output_weight,
):
    rows, width = latent.shape
    chips = tp_size // 2
    local = query_weight.shape[1]
    heads = lambdas.shape[0]
    head = local // heads
    half = head // 2
    plane = 2 * heads
    block_tokens = rows * tp_size
    ctx_rows = context.shape[0]
    piece = modulation.shape[2]
    depth = modulation.shape[1]
    parts = rows // ROWS
    table = tables(sp_size * block_tokens // GRID_W, half)
    vmem = pl.BlockSpec(memory_space=pltpu.VMEM)
    anywhere = pl.BlockSpec(memory_space=pltpu.HBM)
    bf16, f32 = jnp.bfloat16, jnp.float32
    dma = pltpu.SemaphoreType.DMA
    units = (UNITS * chips, rows, width // UNITS)
    return pl.pallas_call(
        functools.partial(block_kernel, sp_size, tp_size),
        out_shape=jax.ShapeDtypeStruct((rows, width), bf16),
        in_specs=[anywhere] * 13,
        out_specs=vmem,
        scratch_shapes=[
            pltpu.VMEM((block_tokens, width), bf16),
            pltpu.VMEM(context.shape, bf16),
            pltpu.VMEM((max(2 * rows, ctx_rows), width), bf16),
            pltpu.VMEM(modulation.shape, bf16),
            pltpu.VMEM((width, local), bf16),
            pltpu.VMEM((width, local), bf16),
            pltpu.VMEM((width, local), bf16),
            pltpu.VMEM((2 * local, width), bf16),
            pltpu.VMEM((sp_size * (ctx_rows + block_tokens), 2 * head), bf16),
            pltpu.VMEM((chips, plane * rows, head), bf16),
            pltpu.VMEM((heads, block_tokens + ctx_rows, 2 * head), bf16),
            pltpu.VMEM((heads, block_tokens, head), bf16),
            pltpu.VMEM((chips, plane * rows, head), bf16),
            pltpu.VMEM((chips, plane, rows, head), bf16),
            pltpu.VMEM(units, f32),
            pltpu.VMEM(units, bf16),
            pltpu.VMEM(units, bf16),
            pltpu.VMEM(units, bf16),
            pltpu.VMEM((sp_size, 8, piece), f32),
            pltpu.VMEM((tp_size, 8, piece), f32),
            pltpu.VMEM((8, width), f32),
            pltpu.VMEM((2, depth), f32),
            pltpu.VMEM(table.shape, f32),
            pltpu.VMEM((block_tokens, half), f32),
            pltpu.VMEM((block_tokens, half), f32),
            pltpu.VMEM((1, head), f32),
            pltpu.VMEM((2, 8, LANES), f32),
            pltpu.VMEM((2,) + row(lambdas).shape, f32),
            pltpu.VMEM((2, plane * rows, head), f32),
            pltpu.VMEM((2, plane * rows, LANES), f32),
            pltpu.VMEM((2, plane * rows, LANES), f32),
            dma((13,)),
            dma((3, chips)),
            dma((parts * tp_size,)),
            dma(()),
            dma((sp_size,)),
            dma(()),
            dma((tp_size,)),
            dma((sp_size,)),
            dma((1,)),
            dma((sp_size, chips + 2)),
            dma((chips + 2,)),
            dma((2 * heads,)),
            dma((plane, chips)),
            dma((plane,)),
            dma((chips, plane)),
            dma((2,)),
            dma((2,)),
            dma((1,)),
            dma((UNITS * chips,)),
            dma((UNITS * chips,)),
        ],
        compiler_params=pltpu.CompilerParams(
            collective_id=0, has_side_effects=True, vmem_limit_bytes=VMEM_LIMIT
        ),
        name="block",
    )(
        *(
            pltpu.with_memory_space_constraint(x, pltpu.HBM)
            for x in (
                latent,
                context,
                row(condition),
                row(context_condition),
                modulation,
                query_weight,
                key_weight,
                value_weight,
                table,
                row(lambdas),
                row(context_lift),
                row(head_gain),
                output_weight,
            )
        )
    )


def solution(mesh):
    in_specs = (
        P(("sp", "tp"), None),
        P("sp", None),
        P(),
        P(),
        P(None, "sp", "tp"),
        P(None, "tp"),
        P(None, "tp"),
        P(None, "tp"),
        P("tp"),
        P("tp"),
        P(),
        P("tp", None),
    )
    out_specs = P(("sp", "tp"), None)
    body = functools.partial(shards, mesh.shape["sp"], mesh.shape["tp"])
    return jax.shard_map(body, mesh=mesh, in_specs=in_specs, out_specs=out_specs, check_vma=False)
```

```python
import functools

import jax
import jax.numpy as jnp
import numpy as np
from jax import lax
from jax.experimental import pallas as pl
from jax.experimental.pallas import tpu as pltpu
from jax.sharding import PartitionSpec as P

GRID_W = 64
ROPE_BASE = 10000.0
EPSILON = 1e-05
LOG2E = 1.4426950408889634
ROWS = 16
LANES = 128
UNITS = 4
VMEM_LIMIT = 53 * 1024 * 1024
MESH = pl.DeviceIdType.MESH


def remote(src, dst, send_sem, recv_sem, **where):
    return pltpu.make_async_remote_copy(
        src_ref=src,
        dst_ref=dst,
        send_sem=send_sem,
        recv_sem=recv_sem,
        device_id=where,
        device_id_type=MESH,
    )


def aligned(start, size, unit):
    return pl.ds(pl.multiple_of(start, unit), size)


def block_kernel(
    sp_size,
    tp_size,
    latent,
    context,
    condition,
    context_condition,
    modulation,
    query_weight,
    key_weight,
    value_weight,
    tables,
    lambdas,
    lift,
    gain_in,
    output_weight,
    result,
    tokens,
    context_tokens,
    normed,
    mod_weight,
    wq,
    wk,
    wv,
    weight,
    keys_values,
    queries,
    kv_stage,
    q_stage,
    out_stage,
    attended,
    own,
    stage,
    incoming,
    lent_blocks,
    mod_parts,
    mod_pieces,
    mod_rows,
    vectors_in,
    table,
    cosine,
    sine,
    gain,
    per_head,
    scalars,
    held,
    held_peak,
    held_sums,
    local_sem,
    tok_send,
    tok_recv,
    part_send,
    part_recv,
    piece_send,
    piece_recv,
    kv_send,
    kv_twin,
    kv_recv,
    kv_pass,
    q_send,
    q_recv,
    out_send,
    out_recv,
    wo_sem,
    head_sem,
    stage_sem,
    left_sem,
    right_sem,
    lend_send,
    lend_recv,
    block_recv,
):
    s = lax.axis_index("sp")
    t = lax.axis_index("tp")
    z = lax.div(t, 2)
    c = lax.rem(t, 2)
    twin = t + 1 - 2 * c
    chips = tp_size // 2
    rows, width = latent.shape
    parts = rows // ROWS
    half_rows = rows // 2
    half_parts = parts // 2
    pair = 2 * rows
    block_tokens = tp_size * rows
    ctx_rows = context.shape[0]
    ctx_total = ctx_rows * sp_size
    local = query_weight.shape[1]
    head = gain_in.shape[1]
    heads = local // head
    half = head // 2
    plane = 2 * heads
    piece = modulation.shape[2]
    depth = modulation.shape[1]
    my_head = lax.rem(s, plane)
    base = s - my_head
    owner_core = lax.div(my_head, heads)
    mine = lax.rem(my_head, heads)
    is_owner = c == owner_core
    ctx_item = 2 * chips

    def load(i, src, dst):
        return pltpu.make_async_copy(src, dst, local_sem.at[i])

    own_slot = tokens.at[aligned(t * rows, rows, ROWS)]
    local_rows = aligned(c * local, local, ROWS)
    here = aligned(s * depth, depth, LANES)
    first_loads = [
        load(0, condition.at[:, here], vectors_in.at[0:1]),
        load(1, context_condition.at[:, here], vectors_in.at[1:2]),
        *(
            load(i, modulation.at[r], mod_weight.at[:depth, r * piece : (r + 1) * piece])
            for r, i in enumerate((2, 13, 14))
        ),
        load(11, lambdas, scalars.at[0]),
        load(12, lift, scalars.at[1]),
    ]
    later_loads = [
        load(3, latent, own_slot),
        load(4, context, context_tokens),
        load(5, key_weight, wk),
        load(6, value_weight, wv),
        load(7, tables, table),
        load(8, query_weight, wq),
        load(9, gain_in, gain),
        load(10, output_weight, weight.at[local_rows]),
    ]
    barrier = pltpu.get_barrier_semaphore()
    for k in range(1, tp_size):
        pl.semaphore_signal(
            barrier, inc=1, device_id={"tp": lax.rem(t + k, tp_size)}, device_id_type=MESH
        )
    for k in range(1, sp_size):
        for to in (t, twin):
            pl.semaphore_signal(
                barrier,
                inc=1,
                device_id={"sp": lax.rem(s + k, sp_size), "tp": to},
                device_id_type=MESH,
            )
    for copy in first_loads + later_loads[:-1]:
        copy.start()
    pl.semaphore_wait(barrier, tp_size - 1 + 2 * (sp_size - 1))

    def token_copy(kind, b, core, part, mine_first=False):
        slot = 2 * b + core
        place = tokens.at[aligned(slot * rows + part * ROWS, ROWS, ROWS)]
        to = (t + 2, t - 2, twin)[kind]
        return remote(
            latent.at[aligned(part * ROWS, ROWS, ROWS)] if mine_first else place,
            place,
            tok_send.at[kind, 0 if kind == 2 else b],
            tok_recv.at[parts * slot + part],
            tp=to,
        )

    def send_mine(part):
        @pl.when(z + 1 < chips)
        def _():
            token_copy(0, z, c, part, True).start()

        @pl.when(z > 0)
        def _():
            token_copy(1, z, c, part, True).start()

        token_copy(2, z, c, part, True).start()

    for part in range(half_parts):
        send_mine(part)

    first_loads[0].wait()
    first_loads[1].wait()
    v = vectors_in[...]
    v = v / (1.0 + jnp.exp(-v))
    which = lax.broadcasted_iota(jnp.int32, (ROWS, depth), 0)
    vectors = jnp.where(
        which == 0,
        jnp.broadcast_to(v[0:1], (ROWS, depth)),
        jnp.broadcast_to(v[1:2], (ROWS, depth)),
    ).astype(jnp.bfloat16)
    first_loads[5].wait()
    first_loads[6].wait()
    for i in range(2):
        for g in range(heads):
            per_head[c, 2 * g + i : 2 * g + i + 1, :] = jnp.broadcast_to(
                scalars[i][:, g : g + 1], (1, LANES)
            )
    for r in range(3):
        first_loads[2 + r].wait()
    for r in range(3):
        found = jnp.dot(
            vectors,
            mod_weight[:depth, r * piece : (r + 1) * piece],
            preferred_element_type=jnp.float32,
        )
        mod_parts[s, 2 * r : 2 * r + 2, :] = found[0:2]
    mod_parts[s, 6:8, :] = jnp.zeros((2, piece), jnp.float32)

    def part_copy(k, owner):
        return remote(
            mod_parts.at[owner],
            mod_parts.at[owner],
            part_send,
            part_recv.at[owner],
            sp=lax.rem(s + k, sp_size),
        )

    def piece_copy(k, owner):
        return remote(
            mod_pieces.at[owner],
            mod_pieces.at[owner],
            piece_send,
            piece_recv.at[owner],
            tp=lax.rem(t + 2 * k, tp_size),
        )

    def piece_across(owner):
        return remote(
            mod_pieces.at[owner],
            mod_pieces.at[owner],
            piece_send,
            piece_recv.at[owner],
            tp=twin,
        )

    def head_copy(core):
        return remote(per_head.at[core], per_head.at[core], head_sem.at[0], head_sem.at[1], tp=twin)

    def weight_copy(core):
        return remote(
            output_weight,
            weight.at[aligned(core * local, local, ROWS)],
            wo_sem.at[0],
            wo_sem.at[1],
            tp=twin,
        )

    for k in range(1, sp_size):
        part_copy(k, s).start()
    head_copy(c).start()
    for k in range(1, sp_size):
        part_copy(k, lax.rem(s + k, sp_size)).wait_recv()
    total = mod_parts[0]
    for i in range(1, sp_size):
        total = total + mod_parts[i]
    mod_pieces[t] = total
    for k in range(1, chips):
        piece_copy(k, t).start()
    piece_across(t).start()
    for part in range(half_parts, parts):
        send_mine(part)
    later_loads[-1].start()
    weight_copy(c).start()

    def forward(d, part):
        left = z - d
        right = z + d

        @pl.when(left >= 0)
        def _():
            token_copy(2, left, c, part).wait_recv()

            @pl.when(z + 1 < chips)
            def _():
                token_copy(0, left, c, part).start()

            token_copy(2, left, c, part).start()

        @pl.when(right < chips)
        def _():
            token_copy(2, right, c, part).wait_recv()

            @pl.when(z > 0)
            def _():
                token_copy(1, right, c, part).start()

            token_copy(2, right, c, part).start()

    for part in range(half_parts):
        forward(1, part)

    grid_rows = block_tokens // GRID_W
    all_rows = table.shape[1] - GRID_W
    later_loads[4].wait()
    is_row = lax.broadcasted_iota(jnp.int32, (GRID_W, half), 1) < half // 2
    for kind, into in enumerate((cosine, sine)):
        by_col = table[kind, all_rows:, :]
        for r in range(grid_rows):
            by_row = table[kind, pl.ds(s * grid_rows + r, 1), :]
            into[r * GRID_W : (r + 1) * GRID_W, :] = jnp.where(is_row, by_row, by_col)

    for k in range(1, chips):
        owner = lax.rem(t + 2 * k, tp_size)
        piece_copy(k, owner).wait_recv()
        piece_across(owner).start()
    for k in range(chips):
        piece_across(lax.rem(twin + 2 * k, tp_size)).wait_recv()

    at_end = (z == 0) | (z + 1 == chips)
    by_end = (z == 1) | (z + 2 == chips)
    inward = jnp.where(z == 0, t + 2, t - 2)
    kept = kept_of(width)

    def lent(core):
        return mod_weight.at[aligned(core * local, local, ROWS), : width - kept]

    lend = remote(
        output_weight.at[:, kept:], lent(c), lend_send.at[0], lend_recv.at[c], tp=inward
    )

    def lend_across(core):
        return remote(lent(core), lent(core), lend_send.at[1], lend_recv.at[core], tp=twin)

    def lend_block(b):
        return remote(
            attended.at[b], lent_blocks.at[b], lend_send.at[2], block_recv.at[b], tp=inward
        )

    @pl.when(at_end)
    def _():
        lend.start()

    for i in range(tp_size):
        found = mod_pieces[i]
        mod_rows[0:2, i * piece : (i + 1) * piece] = found[0:2]
        mod_rows[2:4, i * piece : (i + 1) * piece] = 1.0 + found[2:4]
        mod_rows[4:6, i * piece : (i + 1) * piece] = found[4:6]

    flip = jnp.where(2 * z >= chips, 0, 1)
    near = jnp.minimum(z, chips - 1 - z)
    far = jnp.maximum(z, chips - 1 - z)

    def block_of(i):
        r = jnp.maximum(i - (far - near), 0)
        single = i < far - near
        dist = jnp.where(single, far - i, near - lax.div(r, 2))
        turn_of = jnp.where(single, 0, lax.rem(r, 2))
        pick = turn_of + flip - 2 * turn_of * flip
        return z - dist + 2 * dist * pick

    def arrival(i):
        return block_of(chips - 1 - i)

    def swap(i):
        return jnp.where(i < 2, 1 - i, i) if chips > 2 else i

    tiles = width // LANES

    def normalise(ref, start, count, row):
        def group(g, carry):
            place = aligned(start(g), half_rows, ROWS)

            def tile(i):
                return ref[place, i * LANES : (i + 1) * LANES].astype(jnp.float32)

            sums = tile(0)
            for i in range(1, tiles):
                sums = sums + tile(i)
            center = jnp.sum(sums, axis=1, keepdims=True) * (1.0 / width)
            squares = jnp.zeros((half_rows, LANES), jnp.float32)
            for i in range(tiles):
                x = tile(i) - center
                squares = squares + x * x
            spread = jnp.sum(squares, axis=1, keepdims=True) * (1.0 / width)
            inverse = lax.rsqrt(spread + EPSILON)
            for i in range(tiles):
                cols = slice(i * LANES, (i + 1) * LANES)
                x = (tile(i) - center) * inverse
                y = x * mod_rows[2 + row : 3 + row, cols] + mod_rows[row : row + 1, cols]
                normed[aligned(g * half_rows, half_rows, ROWS), cols] = y.astype(jnp.bfloat16)
            return carry

        lax.fori_loop(0, count, group, 0)

    slots = chips + 2
    early = ctx_total + (chips - 1) * sp_size * pair
    most = early + sp_size * rows

    def size_of(kind):
        return {"block": pair, "half": rows, "context": ctx_rows}[kind]

    def span_of(kind, slot):
        if kind == "context":
            return 0
        if kind == "block":
            return ctx_total + slot * sp_size * pair
        return early + (slot - (chips - 1)) * sp_size * rows

    def kv_place(kind, slot, owner):
        size = size_of(kind)
        return aligned(span_of(kind, slot) + owner * size, size, ROWS)

    def stage_place(kind, slot):
        if kind == "context":
            return pl.ds(block_tokens, ctx_rows)
        start = slot * pair if kind == "block" else (chips - 1) * pair + (slot - chips + 1) * rows
        return aligned(start, size_of(kind), ROWS)

    def kv_copy(k, owner, kind, slot, first=0, last=2):
        cols = pl.ds(first * head, (last - first) * head)
        to = lax.rem(s + k, sp_size)
        return remote(
            kv_stage.at[lax.rem(to, heads), stage_place(kind, slot), cols],
            keys_values.at[kv_place(kind, slot, owner), cols],
            kv_send.at[k],
            kv_recv.at[owner, slot],
            sp=to,
        )

    def wanted(k):
        to = lax.rem(s + k, sp_size)
        return lax.div(lax.rem(to, plane), heads) == c

    def twin_copy(owner, kind, slot):
        place = keys_values.at[kv_place(kind, slot, owner)]
        return remote(place, place, kv_twin.at[0], kv_pass.at[slot], tp=twin)

    def twin_all(kind, slot):
        place = keys_values.at[
            aligned(span_of(kind, slot), sp_size * size_of(kind), ROWS)
        ]
        return remote(place, place, kv_twin.at[0], kv_pass.at[slot], tp=twin)

    def send_kv(kind, slot, first, last):
        for k in range(1, sp_size):

            @pl.when(wanted(k))
            def _():
                kv_copy(k, s, kind, slot, first, last).start()

    def hand_out(find_keys, find_values, kind, slot):
        place = stage_place(kind, slot)
        keys = find_keys()
        for g in range(heads):
            kv_stage[g, place, :head] = keys[:, g * head : (g + 1) * head]
        if kind == "half":
            send_kv(kind, slot, 0, 1)
        values = find_values()
        for g in range(heads):
            kv_stage[g, place, head:] = values[:, g * head : (g + 1) * head]
        send_kv(kind, slot, 1 if kind == "half" else 0, 2)

        @pl.when(is_owner)
        def _():
            keys_values[kv_place(kind, slot, s), :] = kv_stage[mine, place, :]
            twin_copy(s, kind, slot).start()

    def pass_on(kind, slot):
        @pl.when(is_owner)
        def _():
            for k in range(1, sp_size):
                owner = lax.rem(s + k, sp_size)
                kv_copy(k, owner, kind, slot).wait_recv()
                twin_copy(owner, kind, slot).start()

    def take(kind, slot):
        @pl.when(jnp.logical_not(is_owner))
        def _():
            twin_all(kind, slot).wait_recv()

    def q_copy(g, rel, source, b, start, count):
        core = c + rel - 2 * c * rel
        return remote(
            q_stage.at[g, aligned(b * pair + core * rows + start, count, ROWS)],
            queries.at[b, aligned(source * rows + start, count, ROWS)],
            q_send.at[2 * g + rel],
            q_recv.at[source, b],
            sp=base + c * heads + g,
            tp=twin if rel else t,
        )

    def out_copy(b, k, index):
        to = lax.rem(my_head + k, plane)
        return remote(
            out_stage.at[b, aligned(to * rows, rows, ROWS)],
            attended.at[b, index],
            out_send.at[k],
            out_recv.at[b, index],
            sp=base + to,
        )

    quarter = half // 4

    def turn(raw, cos, sin):
        lane = lax.broadcasted_iota(jnp.int32, cos.shape, 1)
        low = lax.rem(lane, 2 * quarter) < quarter
        found = []
        for i in range(local // half):
            v = raw[:, i * half : (i + 1) * half].astype(jnp.bfloat16).astype(jnp.float32)
            other = jnp.where(low, pltpu.roll(v, half - quarter, 1), pltpu.roll(v, quarter, 1))
            found.append((v * cos + other * sin).astype(jnp.bfloat16))
        return jnp.concatenate(found, axis=1)

    def process(b, kind, slot, start):
        count = rows if kind == "block" else half_rows
        first_part = start // ROWS
        for i in range(count // ROWS):
            token_copy(2, b, 1 - c, first_part + i).wait_recv()
        if kind == "block":
            normalise(tokens, lambda g: b * pair + g * half_rows, 4, 0)
        else:
            normalise(tokens, lambda g: b * pair + g * rows + start, 2, 0)

        def of(ref):
            if kind == "block":
                return ref[aligned(b * pair, pair, ROWS), :]
            return jnp.concatenate(
                [
                    ref[aligned(b * pair + core * rows + start, half_rows, ROWS), :]
                    for core in range(2)
                ],
                axis=0,
            )

        cos, sin = of(cosine), of(sine)
        x = normed[: 2 * count, :]
        hand_out(
            lambda: turn(jnp.dot(x, wk[...], preferred_element_type=jnp.float32), cos, sin),
            lambda: jnp.dot(x, wv[...], preferred_element_type=jnp.float32).astype(jnp.bfloat16),
            kind,
            slot,
        )
        turned = turn(jnp.dot(x, wq[...], preferred_element_type=jnp.float32), cos, sin)
        for g in range(heads):
            for core in range(2):
                q_stage[g, aligned(b * pair + core * rows + start, count, ROWS), :] = turned[
                    core * count : (core + 1) * count, g * head : (g + 1) * head
                ]
            q_copy(g, 1, my_head, b, start, count).start()

            @pl.when(c * heads + g != my_head)
            def _():
                q_copy(g, 0, my_head, b, start, count).start()

            @pl.when(c * heads + g == my_head)
            def _():
                queries[b, aligned(my_head * rows + start, count, ROWS), :] = q_stage[
                    g, aligned(b * pair + c * rows + start, count, ROWS), :
                ]

    for i in (1, 2, 3):
        later_loads[i].wait()
    normalise(context_tokens, lambda g: g * half_rows, ctx_rows // half_rows, 1)
    hand_out(
        lambda: jnp.dot(
            normed[:ctx_rows, :], wk[...], preferred_element_type=jnp.float32
        ).astype(jnp.bfloat16),
        lambda: jnp.dot(
            normed[:ctx_rows, :], wv[...], preferred_element_type=jnp.float32
        ).astype(jnp.bfloat16),
        "context",
        slots - 1,
    )
    for part in range(half_parts, parts):
        forward(1, part)
    later_loads[0].wait()
    later_loads[5].wait()

    def forwarded(i):
        dist = jnp.abs(arrival(i) - z)
        ahead = jnp.where(i == 1, half_parts, jnp.where(i == 2, parts - 1, parts))
        return jnp.where(near == 0, dist * parts, jnp.minimum(dist * parts + ahead, far * parts))

    def forward_all(start, stop):
        def one(q, carry):
            forward(1 + lax.div(q, parts), lax.rem(q, parts))
            return carry

        lax.fori_loop(start, stop, one, 0)

    def step(i, done):
        goal = jnp.where(i > 0, jnp.maximum(forwarded(i), done), done)
        forward_all(done, goal)
        process(arrival(i), "block", i, 0)

        @pl.when(i == 0)
        def _():
            pass_on("context", slots - 1)

        @pl.when(i > 0)
        def _():
            pass_on("block", i - 1)

        return goal

    done = lax.fori_loop(0, chips - 1, step, jnp.int32(parts))
    half_way = jnp.maximum(
        done, jnp.where(near == 0, (far - 1) * parts + half_parts, far * parts)
    )
    farthest = arrival(chips - 1)
    forward_all(done, half_way)
    process(farthest, "half", chips - 1, 0)
    pass_on("block", chips - 2)

    tile = plane * rows
    factor = half ** (-0.5) * LOG2E
    head_copy(1 - c).wait_recv()
    later_loads[6].wait()
    weight_of_second = per_head[owner_core, pl.ds(2 * mine, 1), :][:, 0:1]
    raised = per_head[owner_core, pl.ds(2 * mine + 1, 1), :][:, 0:1] * LOG2E

    def partial(b, m, start, stop, lifted):
        scores = (
            lax.dot_general(
                queries[b, :, m * half : (m + 1) * half],
                keys_values[start:stop, m * half : (m + 1) * half],
                (((1,), (1,)), ((), ())),
                preferred_element_type=jnp.float32,
            )
            * factor
        )
        if lifted:
            scores = jnp.concatenate([scores[:, :lifted] + raised, scores[:, lifted:]], axis=1)
        peak = jnp.max(scores, axis=1, keepdims=True)
        weights = jnp.exp2(scores - peak)
        sums = jnp.sum(weights, axis=1, keepdims=True)
        found = jnp.dot(
            weights.astype(jnp.bfloat16),
            keys_values[start:stop, head:],
            preferred_element_type=jnp.float32,
        )
        return peak, sums, found

    def wait_queries(b):
        for k in range(plane):
            source = lax.rem(my_head + k, plane)

            @pl.when(jnp.logical_or(k > 0, jnp.logical_not(is_owner)))
            def _():
                q_copy(0, 0, source, b, 0, rows).wait_recv()

    def begin(b):
        wait_queries(b)
        for m in range(2):
            peak, sums, found = partial(b, m, 0, most, ctx_total)
            held_peak[m] = jnp.broadcast_to(peak, (tile, LANES))
            held_sums[m] = jnp.broadcast_to(sums, (tile, LANES))
            held[m] = found

    def finish(b):
        outs = []
        for m in range(2):
            peak, sums, found = partial(b, m, most, keys_values.shape[0], 0)
            old_peak = held_peak[m][:, 0:1]
            top = jnp.maximum(peak, old_peak)
            now = jnp.exp2(peak - top)
            before = jnp.exp2(old_peak - top)
            sums = sums * now + held_sums[m][:, 0:1] * before
            outs.append((found * now + held[m] * before) / sums)
        hand_back(b, outs)

    def whole(b):
        wait_queries(b)
        outs = []
        for m in range(2):
            _, sums, found = partial(b, m, 0, keys_values.shape[0], ctx_total)
            outs.append(found / sums)
        hand_back(b, outs)

    def hand_back(b, outs):
        diff = outs[0] - weight_of_second * outs[1]
        mean = jnp.sum(diff * diff, axis=1, keepdims=True) * (1.0 / head)
        out_stage[b, :, :] = (diff * lax.rsqrt(mean + EPSILON) * gain[...]).astype(jnp.bfloat16)
        for k in range(1, plane):
            out_copy(b, k, my_head).start()
        attended[b, my_head] = out_stage[b, aligned(my_head * rows, rows, ROWS), :]

    forward_all(half_way, jnp.maximum(half_way, far * parts))
    process(farthest, "half", chips, half_rows)
    pass_on("half", chips - 1)
    take("context", slots - 1)

    def take_block(i, carry):
        take("block", i)
        return carry

    lax.fori_loop(0, chips - 1, take_block, 0)
    take("half", chips - 1)
    begin(block_of(swap(0)))
    pass_on("half", chips)
    take("half", chips)
    finish(block_of(swap(0)))
    weight_copy(1 - c).wait_recv()
    later_loads[7].wait()

    sizes = (kept // 2, (width - kept) // 2)

    def columns(kind, n):
        start = n * sizes[0] if kind == 0 else kept + (n - 2) * sizes[1]
        return aligned(start, sizes[kind], LANES)

    def right_copy(b, kind, n):
        cols = columns(kind, n)
        return remote(
            stage.at[b, :, cols],
            incoming.at[b + 1, :, cols],
            stage_sem.at[0],
            left_sem.at[b * UNITS + n],
            tp=t + 2,
        )

    def left_copy(b, kind, n):
        cols = columns(kind, n)
        return remote(
            stage.at[b, :, cols],
            incoming.at[b, :, cols],
            stage_sem.at[0],
            right_sem.at[b * UNITS + n],
            tp=t - 2,
        )

    def rows_of(ref, b):
        return jnp.concatenate([ref[b, g] for g in range(plane)], axis=1)

    def borrowed(b, n):
        if isinstance(n, int):
            if n == 2:
                lend_block(b).wait_recv()
        else:

            @pl.when(n == 2)
            def _():
                lend_block(b).wait_recv()

        return jnp.dot(
            rows_of(lent_blocks, b),
            mod_weight[: 2 * local, aligned((n - 2) * sizes[1], sizes[1], LANES)],
            preferred_element_type=jnp.float32,
        )

    def unit_at(q):
        index, n = lax.div(q, UNITS), lax.rem(q, UNITS)
        n = jnp.where(n == 0, 2, jnp.where(n == 3, 3, n - 1))
        for place, (i, piece_of) in enumerate(
            [(0, 0), (0, 2), (1, 2), (1, 0), (1, 1), (1, 3), (0, 1), (0, 3)]
        ):
            index = jnp.where(q == place, i, index)
            n = jnp.where(q == place, piece_of, n)
        return swap(index), n

    def send_sums(b, n):
        @pl.when(z == 0)
        def _():
            right_copy(b, 0, n).start()

        @pl.when(z > 0)
        def _():
            left_copy(b, 0, n).start()

    def project(i):
        b = block_of(swap(i))
        for k in range(1, plane):
            out_copy(b, k, lax.rem(my_head + k, plane)).wait_recv()
        sends = at_end & (b != z)

        @pl.when(sends)
        def _():
            lend_block(b).start()

        x = rows_of(attended, b)
        for n in range(UNITS):
            kind = n // 2
            start = n * sizes[0] if kind == 0 else kept + (n - 2) * sizes[1]
            cols = slice(start, start + sizes[kind])

            def find():
                return jnp.dot(x, weight[:, cols], preferred_element_type=jnp.float32)

            if kind == 0:
                found = find()
                own[b, :, cols] = found

                @pl.when(sends)
                def _():
                    stage[b, :, cols] = found.astype(jnp.bfloat16)

                    @pl.when((i > 0) | (n == 0))
                    def _():
                        send_sums(b, n)
            else:

                @pl.when(jnp.logical_not(sends))
                def _():
                    own[b, :, cols] = find()

        @pl.when(at_end & (i == 1))
        def _():
            send_sums(block_of(swap(0)), 1)

    hop = 2

    def combine_one(b, n, wanted_here, copy, slot, neighbour):
        for kind in range(2):
            cols = columns(kind, n)
            here = wanted_here & (lax.div(n, 2) == kind)
            received = here & jnp.logical_not(neighbour) if kind else here

            @pl.when(received)
            def _():
                copy(b, kind, n).wait_recv()
                stage[b, :, cols] = (
                    own[b, :, cols] + incoming[slot, :, cols].astype(jnp.float32)
                ).astype(jnp.bfloat16)
                copy(b, kind, n).start()

            if kind:

                @pl.when(here & neighbour)
                def _():
                    stage[b, :, cols] = (own[b, :, cols] + borrowed(b, n)).astype(jnp.bfloat16)
                    copy(b, kind, n).start()

    def combine_step(i, carry):
        q = jnp.maximum(i - hop * (chips - 1 - z), 0)
        b, n = unit_at(q)
        here = (i >= hop * (chips - 1 - z)) & (b < z)
        combine_one(b, n, here, left_copy, b, z + 2 == chips)
        p = jnp.maximum(i - hop * z, 0)
        e, n = unit_at(p)
        e = chips - 1 - e
        here = (i >= hop * z) & (e > z)
        combine_one(e, n, here, right_copy, e + 1, z == 1)
        return carry

    def combine(start, stop):
        @pl.when(jnp.logical_not(at_end))
        def _():
            lax.fori_loop(start, stop, combine_step, 0)

    steps = 2 * chips - 1

    def attend_step(k, carry):
        index = lax.div(k, 2)
        attends = (lax.rem(k, 2) == 0) & (k + 1 < steps)

        @pl.when(attends)
        def _():
            whole(block_of(swap(index + 1)))

        @pl.when(jnp.logical_not(attends))
        def _():
            project(index)

        @pl.when((k == 3) & by_end)
        def _():
            lend.wait_recv()
            lend_across(c).start()

        @pl.when(k == steps - 3)
        def _():
            combine(0, hop + 1)

        @pl.when((k == steps - 2) & by_end)
        def _():
            lend_across(1 - c).wait_recv()

        @pl.when(k == steps - 2)
        def _():
            combine(hop + 1, hop + 2)

        return carry

    lax.fori_loop(0, steps, attend_step, 0)

    def copies_left():
        for k in range(1, plane):
            remote(
                attended.at[:, 0], attended.at[:, 0], out_send.at[k], out_recv.at[0, 0], tp=twin
            ).wait_send()

        def sent_tokens(b, carry):
            place = tokens.at[aligned(b * rows, rows, ROWS)]

            @pl.when((b <= z) & (z + 1 < chips))
            def _():
                remote(place, place, tok_send.at[0, b], tok_recv.at[0], tp=twin).wait_send()

            @pl.when((b >= z) & (z > 0))
            def _():
                remote(place, place, tok_send.at[1, b], tok_recv.at[0], tp=twin).wait_send()

            return carry

        lax.fori_loop(0, chips, sent_tokens, 0)
        place = tokens.at[: chips * rows]
        remote(place, place, tok_send.at[2, 0], tok_recv.at[0], tp=twin).wait_send()
        for g in range(heads):
            place = q_stage.at[g, : chips * rows]
            remote(place, place, q_send.at[2 * g + 1], q_recv.at[0, 0], tp=twin).wait_send()

            @pl.when(c * heads + g != my_head)
            def _():
                remote(place, place, q_send.at[2 * g], q_recv.at[0, 0], tp=twin).wait_send()

        for k in range(1, sp_size):

            @pl.when(wanted(k))
            def _():
                place = kv_stage.at[0]
                remote(place, place, kv_send.at[k], kv_recv.at[0, 0], tp=twin).wait_send()

        @pl.when(is_owner)
        def _():
            remote(
                keys_values, keys_values, kv_twin.at[0], kv_pass.at[0], tp=twin
            ).wait_send()

        place = mod_parts.at[: sp_size - 1]
        remote(place, place, part_send, part_recv.at[0], tp=twin).wait_send()
        place = mod_pieces.at[: tp_size - 1]
        remote(place, place, piece_send, piece_recv.at[0], tp=twin).wait_send()
        head_copy(c).wait_send()
        weight_copy(c).wait_send()

    copies_left()
    combine(hop + 2, (chips - 1) * (UNITS + hop))

    for n in range(UNITS):
        kind = n // 2
        start = n * sizes[0] if kind == 0 else kept + (n - 2) * sizes[1]
        cols = slice(start, start + sizes[kind])

        def add(copy, slot, present, neighbour):
            received = present & jnp.logical_not(neighbour) if kind else present

            @pl.when(received)
            def _():
                copy(z, kind, n).wait_recv()
                own[z, :, cols] = own[z, :, cols] + incoming[slot, :, cols].astype(jnp.float32)

            if kind:

                @pl.when(neighbour)
                def _():
                    own[z, :, cols] = own[z, :, cols] + borrowed(z, n)

        add(right_copy, z + 1, z > 0, z == 1)
        add(left_copy, z, z + 1 < chips, z + 2 == chips)
        result[:, cols] = (
            tokens[aligned(t * rows, rows, ROWS), cols].astype(jnp.float32)
            + mod_rows[4:5, cols] * own[z, :, cols]
        ).astype(jnp.bfloat16)

    @pl.when(at_end)
    def _():
        place = stage.at[: chips - 1, :, :kept]
        remote(place, place, stage_sem.at[0], left_sem.at[0], tp=twin).wait_send()
        lend.wait_send()
        place = attended.at[: chips - 1]
        remote(place, place, lend_send.at[2], block_recv.at[0], tp=twin).wait_send()

    @pl.when(jnp.logical_not(at_end))
    def _():
        place = stage.at[: chips - 1]
        remote(place, place, stage_sem.at[0], left_sem.at[0], tp=twin).wait_send()

    @pl.when(by_end)
    def _():
        lend_across(c).wait_send()


def kept_of(width):
    return width * 5 // 8


def tables(grid_rows, half):
    quarter = half // 4
    inverse = (ROPE_BASE ** (-np.arange(quarter) / quarter)).astype(np.float32)
    sign = np.where(np.arange(half) % (2 * quarter) < quarter, -1.0, 1.0)
    places = np.concatenate([np.arange(grid_rows), np.arange(GRID_W)]).astype(np.float32)
    angles = (places[:, None] * np.tile(inverse, 4)).astype(np.float64)
    return np.stack([np.cos(angles), np.sin(angles) * sign]).astype(np.float32)


def row(x):
    return x.reshape(1, -1) if x.size > 1 else jnp.broadcast_to(x.reshape(1, 1), (1, LANES))


def shards(
    sp_size,
    tp_size,
    latent,
    context,
    condition,
    context_condition,
    modulation,
    query_weight,
    key_weight,
    value_weight,
    lambdas,
    context_lift,
    head_gain,
    output_weight,
):
    rows, width = latent.shape
    chips = tp_size // 2
    local = query_weight.shape[1]
    heads = lambdas.shape[0]
    head = local // heads
    half = head // 2
    plane = 2 * heads
    block_tokens = rows * tp_size
    ctx_rows = context.shape[0]
    piece = modulation.shape[2]
    depth = modulation.shape[1]
    parts = rows // ROWS
    table = tables(sp_size * block_tokens // GRID_W, half)
    vmem = pl.BlockSpec(memory_space=pltpu.VMEM)
    anywhere = pl.BlockSpec(memory_space=pltpu.HBM)
    bf16, f32 = jnp.bfloat16, jnp.float32
    dma = pltpu.SemaphoreType.DMA
    blocks = (chips, rows, width)
    return pl.pallas_call(
        functools.partial(block_kernel, sp_size, tp_size),
        out_shape=jax.ShapeDtypeStruct((rows, width), bf16),
        in_specs=[anywhere] * 13,
        out_specs=vmem,
        scratch_shapes=[
            pltpu.VMEM((block_tokens, width), bf16),
            pltpu.VMEM(context.shape, bf16),
            pltpu.VMEM((max(2 * rows, ctx_rows), width), bf16),
            pltpu.VMEM((max(depth, 2 * local), max(3 * piece, width - kept_of(width))), bf16),
            pltpu.VMEM((width, local), bf16),
            pltpu.VMEM((width, local), bf16),
            pltpu.VMEM((width, local), bf16),
            pltpu.VMEM((2 * local, width), bf16),
            pltpu.VMEM((sp_size * (ctx_rows + block_tokens), 2 * head), bf16),
            pltpu.VMEM((chips, plane * rows, head), bf16),
            pltpu.VMEM((heads, block_tokens + ctx_rows, 2 * head), bf16),
            pltpu.VMEM((heads, block_tokens, head), bf16),
            pltpu.VMEM((chips, plane * rows, head), bf16),
            pltpu.VMEM((chips, plane, rows, head), bf16),
            pltpu.VMEM(blocks, f32),
            pltpu.VMEM(blocks, bf16),
            pltpu.VMEM((chips + 1, rows, width), bf16),
            pltpu.VMEM((chips, plane, rows, head), bf16),
            pltpu.VMEM((sp_size, 8, piece), f32),
            pltpu.VMEM((tp_size, 8, piece), f32),
            pltpu.VMEM((8, width), f32),
            pltpu.VMEM((2, depth), f32),
            pltpu.VMEM(table.shape, f32),
            pltpu.VMEM((block_tokens, half), f32),
            pltpu.VMEM((block_tokens, half), f32),
            pltpu.VMEM((1, head), f32),
            pltpu.VMEM((2, 8, LANES), f32),
            pltpu.VMEM((2,) + row(lambdas).shape, f32),
            pltpu.VMEM((2, plane * rows, head), f32),
            pltpu.VMEM((2, plane * rows, LANES), f32),
            pltpu.VMEM((2, plane * rows, LANES), f32),
            dma((15,)),
            dma((3, chips)),
            dma((parts * tp_size,)),
            dma(()),
            dma((sp_size,)),
            dma(()),
            dma((tp_size,)),
            dma((sp_size,)),
            dma((1,)),
            dma((sp_size, chips + 2)),
            dma((chips + 2,)),
            dma((2 * heads,)),
            dma((plane, chips)),
            dma((plane,)),
            dma((chips, plane)),
            dma((2,)),
            dma((2,)),
            dma((1,)),
            dma((UNITS * chips,)),
            dma((UNITS * chips,)),
            dma((3,)),
            dma((2,)),
            dma((chips,)),
        ],
        compiler_params=pltpu.CompilerParams(
            collective_id=0, has_side_effects=True, vmem_limit_bytes=VMEM_LIMIT
        ),
        name="block",
    )(
        *(
            pltpu.with_memory_space_constraint(x, pltpu.HBM)
            for x in (
                latent,
                context,
                row(condition),
                row(context_condition),
                modulation,
                query_weight,
                key_weight,
                value_weight,
                table,
                row(lambdas),
                row(context_lift),
                row(head_gain),
                output_weight,
            )
        )
    )


def solution(mesh):
    in_specs = (
        P(("sp", "tp"), None),
        P("sp", None),
        P(),
        P(),
        P(None, "sp", "tp"),
        P(None, "tp"),
        P(None, "tp"),
        P(None, "tp"),
        P("tp"),
        P("tp"),
        P(),
        P("tp", None),
    )
    out_specs = P(("sp", "tp"), None)
    body = functools.partial(shards, mesh.shape["sp"], mesh.shape["tp"])
    return jax.shard_map(body, mesh=mesh, in_specs=in_specs, out_specs=out_specs, check_vma=False)
```

```python
import functools

import jax
import jax.numpy as jnp
import numpy as np
from jax import lax
from jax.experimental import pallas as pl
from jax.experimental.pallas import tpu as pltpu
from jax.sharding import PartitionSpec as P

GRID_W = 64
ROPE_BASE = 10000.0
EPSILON = 1e-05
LOG2E = 1.4426950408889634
ROWS = 16
LANES = 128
UNITS = 4
VMEM_LIMIT = 53 * 1024 * 1024
MESH = pl.DeviceIdType.MESH


def remote(src, dst, send_sem, recv_sem, **where):
    return pltpu.make_async_remote_copy(
        src_ref=src,
        dst_ref=dst,
        send_sem=send_sem,
        recv_sem=recv_sem,
        device_id=where,
        device_id_type=MESH,
    )


def aligned(start, size, unit):
    return pl.ds(pl.multiple_of(start, unit), size)


def block_kernel(
    sp_size,
    tp_size,
    latent,
    context,
    condition,
    context_condition,
    modulation,
    query_weight,
    key_weight,
    value_weight,
    tables,
    lambdas,
    lift,
    gain_in,
    output_weight,
    result,
    tokens,
    context_tokens,
    normed,
    mod_weight,
    wq,
    wk,
    wv,
    weight,
    keys_values,
    queries,
    kv_stage,
    q_stage,
    out_stage,
    attended,
    own,
    stage,
    incoming,
    lent_blocks,
    mod_parts,
    mod_pieces,
    mod_rows,
    vectors_in,
    table,
    cosine,
    sine,
    gain,
    per_head,
    scalars,
    held,
    held_peak,
    held_sums,
    local_sem,
    tok_send,
    tok_recv,
    twin_recv,
    part_send,
    part_recv,
    piece_send,
    piece_recv,
    kv_send,
    kv_twin,
    kv_recv,
    kv_pass,
    q_send,
    q_recv,
    out_send,
    out_recv,
    wo_sem,
    head_sem,
    stage_sem,
    sums_sem,
    lend_send,
    lend_recv,
    block_recv,
):
    s = lax.axis_index("sp")
    t = lax.axis_index("tp")
    z = lax.div(t, 2)
    c = lax.rem(t, 2)
    twin = t + 1 - 2 * c
    chips = tp_size // 2
    rows, width = latent.shape
    parts = rows // ROWS
    half_rows = rows // 2
    half_parts = parts // 2
    pair = 2 * rows
    block_tokens = tp_size * rows
    ctx_rows = context.shape[0]
    ctx_total = ctx_rows * sp_size
    local = query_weight.shape[1]
    head = gain_in.shape[1]
    heads = local // head
    half = head // 2
    plane = 2 * heads
    piece = modulation.shape[2]
    depth = modulation.shape[1]
    my_head = lax.rem(s, plane)
    base = s - my_head
    owner_core = lax.div(my_head, heads)
    mine = lax.rem(my_head, heads)
    is_owner = c == owner_core
    ctx_item = 2 * chips

    def load(i, src, dst):
        return pltpu.make_async_copy(src, dst, local_sem.at[i])

    own_slot = tokens.at[aligned(t * rows, rows, ROWS)]
    local_rows = aligned(c * local, local, ROWS)
    here = aligned(s * depth, depth, LANES)
    first_loads = [
        load(0, condition.at[:, here], vectors_in.at[0:1]),
        load(1, context_condition.at[:, here], vectors_in.at[1:2]),
        *(
            load(i, modulation.at[r], mod_weight.at[:depth, r * piece : (r + 1) * piece])
            for r, i in enumerate((2, 13, 14))
        ),
        load(11, lambdas, scalars.at[0]),
        load(12, lift, scalars.at[1]),
    ]
    later_loads = [
        load(3, latent, own_slot),
        load(4, context, context_tokens),
        load(5, key_weight, wk),
        load(6, value_weight, wv),
        load(7, tables, table),
        load(8, query_weight, wq),
        load(9, gain_in, gain),
        load(10, output_weight, weight.at[local_rows]),
    ]
    barrier = pltpu.get_barrier_semaphore()
    for k in range(1, tp_size):
        pl.semaphore_signal(
            barrier, inc=1, device_id={"tp": lax.rem(t + k, tp_size)}, device_id_type=MESH
        )
    for k in range(1, sp_size):
        for to in (t, twin):
            pl.semaphore_signal(
                barrier,
                inc=1,
                device_id={"sp": lax.rem(s + k, sp_size), "tp": to},
                device_id_type=MESH,
            )
    for copy in first_loads + later_loads[:-1]:
        copy.start()
    pl.semaphore_wait(barrier, tp_size - 1 + 2 * (sp_size - 1))

    def token_copy(kind, b, core, part, mine_first=False):
        slot = 2 * b + core
        place = tokens.at[aligned(slot * rows + part * ROWS, ROWS, ROWS)]
        to = (t + 2, t - 2, twin)[kind]
        return remote(
            latent.at[aligned(part * ROWS, ROWS, ROWS)] if mine_first else place,
            place,
            tok_send.at[kind, 0 if kind == 2 else b],
            twin_recv.at[2 * b + lax.div(part, half_parts)] if kind == 2 else tok_recv.at[parts * b + part],
            tp=to,
        )

    def send_mine(part):
        @pl.when(z + 1 < chips)
        def _():
            token_copy(0, z, c, part, True).start()

        @pl.when(z > 0)
        def _():
            token_copy(1, z, c, part, True).start()

        token_copy(2, z, c, part, True).start()

    for part in range(half_parts):
        send_mine(part)

    first_loads[0].wait()
    first_loads[1].wait()
    v = vectors_in[...]
    v = v / (1.0 + jnp.exp(-v))
    which = lax.broadcasted_iota(jnp.int32, (ROWS, depth), 0)
    vectors = jnp.where(
        which == 0,
        jnp.broadcast_to(v[0:1], (ROWS, depth)),
        jnp.broadcast_to(v[1:2], (ROWS, depth)),
    ).astype(jnp.bfloat16)
    first_loads[5].wait()
    first_loads[6].wait()
    for i in range(2):
        for g in range(heads):
            per_head[c, 2 * g + i : 2 * g + i + 1, :] = jnp.broadcast_to(
                scalars[i][:, g : g + 1], (1, LANES)
            )
    for r in range(3):
        first_loads[2 + r].wait()
    for r in range(3):
        found = jnp.dot(
            vectors,
            mod_weight[:depth, r * piece : (r + 1) * piece],
            preferred_element_type=jnp.float32,
        )
        mod_parts[s, 2 * r : 2 * r + 2, :] = found[0:2]
    mod_parts[s, 6:8, :] = jnp.zeros((2, piece), jnp.float32)

    def part_copy(k, owner):
        return remote(
            mod_parts.at[owner],
            mod_parts.at[owner],
            part_send,
            part_recv,
            sp=lax.rem(s + k, sp_size),
        )

    def piece_copy(k, owner):
        return remote(
            mod_pieces.at[owner],
            mod_pieces.at[owner],
            piece_send,
            piece_recv.at[owner],
            tp=lax.rem(t + 2 * k, tp_size),
        )

    def piece_across(owner):
        return remote(
            mod_pieces.at[owner],
            mod_pieces.at[owner],
            piece_send,
            piece_recv.at[owner],
            tp=twin,
        )

    def head_copy(core):
        return remote(per_head.at[core], per_head.at[core], head_sem.at[0], head_sem.at[1], tp=twin)

    def weight_copy(core):
        return remote(
            output_weight,
            weight.at[aligned(core * local, local, ROWS)],
            wo_sem.at[0],
            wo_sem.at[1],
            tp=twin,
        )

    for k in range(1, sp_size):
        part_copy(k, s).start()
    head_copy(c).start()
    place = mod_parts.at[: sp_size - 1]
    remote(place, place, part_send, part_recv, tp=twin).wait_recv()
    total = mod_parts[0]
    for i in range(1, sp_size):
        total = total + mod_parts[i]
    mod_pieces[t] = total
    for k in range(1, chips):
        piece_copy(k, t).start()
    piece_across(t).start()
    for part in range(half_parts, parts):
        send_mine(part)
    later_loads[-1].start()
    weight_copy(c).start()

    def forward(d, part):
        left = z - d
        right = z + d

        @pl.when(left >= 0)
        def _():
            token_copy(0, left, c, part).wait_recv()

            @pl.when(z + 1 < chips)
            def _():
                token_copy(0, left, c, part).start()

            token_copy(2, left, c, part).start()

        @pl.when(right < chips)
        def _():
            token_copy(1, right, c, part).wait_recv()

            @pl.when(z > 0)
            def _():
                token_copy(1, right, c, part).start()

            token_copy(2, right, c, part).start()

    for part in range(half_parts):
        forward(1, part)

    grid_rows = block_tokens // GRID_W
    all_rows = table.shape[1] - GRID_W
    later_loads[4].wait()
    is_row = lax.broadcasted_iota(jnp.int32, (GRID_W, half), 1) < half // 2
    for kind, into in enumerate((cosine, sine)):
        by_col = table[kind, all_rows:, :]
        for r in range(grid_rows):
            by_row = table[kind, pl.ds(s * grid_rows + r, 1), :]
            into[r * GRID_W : (r + 1) * GRID_W, :] = jnp.where(is_row, by_row, by_col)

    for k in range(1, chips):
        owner = lax.rem(t + 2 * k, tp_size)
        piece_copy(k, owner).wait_recv()
        piece_across(owner).start()
    for k in range(chips):
        piece_across(lax.rem(twin + 2 * k, tp_size)).wait_recv()

    at_end = (z == 0) | (z + 1 == chips)
    by_end = (z == 1) | (z + 2 == chips)
    inward = jnp.where(z == 0, t + 2, t - 2)
    kept = kept_of(width)

    def lent(core):
        return mod_weight.at[aligned(core * local, local, ROWS), : width - kept]

    lend = remote(
        output_weight.at[:, kept:], lent(c), lend_send.at[0], lend_recv.at[c], tp=inward
    )

    def lend_across(core):
        return remote(lent(core), lent(core), lend_send.at[1], lend_recv.at[core], tp=twin)

    def lend_block(b):
        return remote(
            attended.at[b], lent_blocks.at[b], lend_send.at[2], block_recv.at[b], tp=inward
        )

    @pl.when(at_end)
    def _():
        lend.start()

    for i in range(tp_size):
        found = mod_pieces[i]
        mod_rows[0:2, i * piece : (i + 1) * piece] = found[0:2]
        mod_rows[2:4, i * piece : (i + 1) * piece] = 1.0 + found[2:4]
        mod_rows[4:6, i * piece : (i + 1) * piece] = found[4:6]

    flip = jnp.where(2 * z >= chips, 0, 1)
    near = jnp.minimum(z, chips - 1 - z)
    far = jnp.maximum(z, chips - 1 - z)

    def block_of(i):
        r = jnp.maximum(i - (far - near), 0)
        single = i < far - near
        dist = jnp.where(single, far - i, near - lax.div(r, 2))
        turn_of = jnp.where(single, 0, lax.rem(r, 2))
        pick = turn_of + flip - 2 * turn_of * flip
        return z - dist + 2 * dist * pick

    def arrival(i):
        return block_of(chips - 1 - i)

    def swap(i):
        return jnp.where(i < 2, 1 - i, i) if chips > 2 else i

    tiles = width // LANES

    def normalise(ref, start, count, row):
        def group(g, carry):
            place = aligned(start(g), half_rows, ROWS)

            def tile(i):
                return ref[place, i * LANES : (i + 1) * LANES].astype(jnp.float32)

            sums = tile(0)
            for i in range(1, tiles):
                sums = sums + tile(i)
            center = jnp.sum(sums, axis=1, keepdims=True) * (1.0 / width)
            squares = jnp.zeros((half_rows, LANES), jnp.float32)
            for i in range(tiles):
                x = tile(i) - center
                squares = squares + x * x
            spread = jnp.sum(squares, axis=1, keepdims=True) * (1.0 / width)
            inverse = lax.rsqrt(spread + EPSILON)
            for i in range(tiles):
                cols = slice(i * LANES, (i + 1) * LANES)
                x = (tile(i) - center) * inverse
                y = x * mod_rows[2 + row : 3 + row, cols] + mod_rows[row : row + 1, cols]
                normed[aligned(g * half_rows, half_rows, ROWS), cols] = y.astype(jnp.bfloat16)
            return carry

        lax.fori_loop(0, count, group, 0)

    slots = chips + 2
    early = ctx_total + (chips - 1) * sp_size * pair
    most = early + sp_size * rows

    def size_of(kind):
        return {"block": pair, "half": rows, "context": ctx_rows}[kind]

    def span_of(kind, slot):
        if kind == "context":
            return 0
        if kind == "block":
            return ctx_total + slot * sp_size * pair
        return early + (slot - (chips - 1)) * sp_size * rows

    def kv_place(kind, slot, owner):
        size = size_of(kind)
        return aligned(span_of(kind, slot) + owner * size, size, ROWS)

    def stage_place(kind, slot):
        if kind == "context":
            return pl.ds(block_tokens, ctx_rows)
        start = slot * pair if kind == "block" else (chips - 1) * pair + (slot - chips + 1) * rows
        return aligned(start, size_of(kind), ROWS)

    def kv_copy(k, owner, kind, slot, first=0, last=2):
        cols = pl.ds(first * head, (last - first) * head)
        to = lax.rem(s + k, sp_size)
        return remote(
            kv_stage.at[lax.rem(to, heads), stage_place(kind, slot), cols],
            keys_values.at[kv_place(kind, slot, owner), cols],
            kv_send.at[k],
            kv_recv.at[slot],
            sp=to,
        )

    def wanted(k):
        to = lax.rem(s + k, sp_size)
        return lax.div(lax.rem(to, plane), heads) == c

    def twin_copy(owner, kind, slot):
        place = keys_values.at[kv_place(kind, slot, owner)]
        return remote(place, place, kv_twin.at[0], kv_pass.at[slot], tp=twin)

    def twin_all(kind, slot):
        place = keys_values.at[
            aligned(span_of(kind, slot), sp_size * size_of(kind), ROWS)
        ]
        return remote(place, place, kv_twin.at[0], kv_pass.at[slot], tp=twin)

    def send_kv(kind, slot, first, last):
        for k in range(1, sp_size):

            @pl.when(wanted(k))
            def _():
                kv_copy(k, s, kind, slot, first, last).start()

    def hand_out(find_keys, find_values, kind, slot):
        place = stage_place(kind, slot)
        keys = find_keys()
        for g in range(heads):
            kv_stage[g, place, :head] = keys[:, g * head : (g + 1) * head]
        if kind == "half":
            send_kv(kind, slot, 0, 1)
        values = find_values()
        for g in range(heads):
            kv_stage[g, place, head:] = values[:, g * head : (g + 1) * head]
        send_kv(kind, slot, 1 if kind == "half" else 0, 2)

        @pl.when(is_owner)
        def _():
            keys_values[kv_place(kind, slot, s), :] = kv_stage[mine, place, :]
            twin_copy(s, kind, slot).start()

    def pass_on(kind, slot):
        @pl.when(is_owner)
        def _():
            place = keys_values.at[: (sp_size - 1) * size_of(kind)]
            remote(place, place, kv_send.at[0], kv_recv.at[slot], tp=twin).wait_recv()
            for k in range(1, sp_size):
                twin_copy(lax.rem(s + k, sp_size), kind, slot).start()

    def take(kind, slot):
        @pl.when(jnp.logical_not(is_owner))
        def _():
            twin_all(kind, slot).wait_recv()

    def q_copy(g, rel, source, b, start, count):
        core = c + rel - 2 * c * rel
        return remote(
            q_stage.at[g, aligned(b * pair + core * rows + start, count, ROWS)],
            queries.at[b, aligned(source * rows + start, count, ROWS)],
            q_send.at[2 * g + rel],
            q_recv.at[b],
            sp=base + c * heads + g,
            tp=twin if rel else t,
        )

    def out_copy(b, k, index):
        to = lax.rem(my_head + k, plane)
        return remote(
            out_stage.at[b, aligned(to * rows, rows, ROWS)],
            attended.at[b, index],
            out_send.at[k],
            out_recv.at[b],
            sp=base + to,
        )

    quarter = half // 4

    def turn(raw, cos, sin):
        lane = lax.broadcasted_iota(jnp.int32, cos.shape, 1)
        low = lax.rem(lane, 2 * quarter) < quarter
        found = []
        for i in range(local // half):
            v = raw[:, i * half : (i + 1) * half].astype(jnp.bfloat16).astype(jnp.float32)
            other = jnp.where(low, pltpu.roll(v, half - quarter, 1), pltpu.roll(v, quarter, 1))
            found.append((v * cos + other * sin).astype(jnp.bfloat16))
        return jnp.concatenate(found, axis=1)

    def process(b, kind, slot, start):
        count = rows if kind == "block" else half_rows
        first_part = start // ROWS
        for i in range(count // half_rows):
            place = tokens.at[:half_rows]
            arrived = twin_recv.at[2 * b + lax.div(first_part, half_parts) + i]
            remote(place, place, tok_send.at[2, 0], arrived, tp=twin).wait_recv()
        if kind == "block":
            normalise(tokens, lambda g: b * pair + g * half_rows, 4, 0)
        else:
            normalise(tokens, lambda g: b * pair + g * rows + start, 2, 0)

        def of(ref):
            if kind == "block":
                return ref[aligned(b * pair, pair, ROWS), :]
            return jnp.concatenate(
                [
                    ref[aligned(b * pair + core * rows + start, half_rows, ROWS), :]
                    for core in range(2)
                ],
                axis=0,
            )

        cos, sin = of(cosine), of(sine)
        x = normed[: 2 * count, :]
        hand_out(
            lambda: turn(jnp.dot(x, wk[...], preferred_element_type=jnp.float32), cos, sin),
            lambda: jnp.dot(x, wv[...], preferred_element_type=jnp.float32).astype(jnp.bfloat16),
            kind,
            slot,
        )
        turned = turn(jnp.dot(x, wq[...], preferred_element_type=jnp.float32), cos, sin)
        for g in range(heads):
            for core in range(2):
                q_stage[g, aligned(b * pair + core * rows + start, count, ROWS), :] = turned[
                    core * count : (core + 1) * count, g * head : (g + 1) * head
                ]
            q_copy(g, 1, my_head, b, start, count).start()

            @pl.when(c * heads + g != my_head)
            def _():
                q_copy(g, 0, my_head, b, start, count).start()

            @pl.when(c * heads + g == my_head)
            def _():
                queries[b, aligned(my_head * rows + start, count, ROWS), :] = q_stage[
                    g, aligned(b * pair + c * rows + start, count, ROWS), :
                ]

    for i in (1, 2, 3):
        later_loads[i].wait()
    normalise(context_tokens, lambda g: g * half_rows, ctx_rows // half_rows, 1)
    hand_out(
        lambda: jnp.dot(
            normed[:ctx_rows, :], wk[...], preferred_element_type=jnp.float32
        ).astype(jnp.bfloat16),
        lambda: jnp.dot(
            normed[:ctx_rows, :], wv[...], preferred_element_type=jnp.float32
        ).astype(jnp.bfloat16),
        "context",
        slots - 1,
    )
    for part in range(half_parts, parts):
        forward(1, part)
    later_loads[0].wait()
    later_loads[5].wait()

    def forwarded(i):
        dist = jnp.abs(arrival(i) - z)
        ahead = jnp.where(i == 1, half_parts, jnp.where(i == 2, parts - 1, parts))
        return jnp.where(near == 0, dist * parts, jnp.minimum(dist * parts + ahead, far * parts))

    def forward_all(start, stop):
        def one(q, carry):
            forward(1 + lax.div(q, parts), lax.rem(q, parts))
            return carry

        lax.fori_loop(start, stop, one, 0)

    def step(i, done):
        goal = jnp.where(i > 0, jnp.maximum(forwarded(i), done), done)
        forward_all(done, goal)
        process(arrival(i), "block", i, 0)

        @pl.when(i == 0)
        def _():
            pass_on("context", slots - 1)

        @pl.when(i > 0)
        def _():
            pass_on("block", i - 1)

        return goal

    done = lax.fori_loop(0, chips - 1, step, jnp.int32(parts))
    half_way = jnp.maximum(
        done, jnp.where(near == 0, (far - 1) * parts + half_parts, far * parts)
    )
    farthest = arrival(chips - 1)
    forward_all(done, half_way)
    process(farthest, "half", chips - 1, 0)
    pass_on("block", chips - 2)

    tile = plane * rows
    factor = half ** (-0.5) * LOG2E
    head_copy(1 - c).wait_recv()
    later_loads[6].wait()
    weight_of_second = per_head[owner_core, pl.ds(2 * mine, 1), :][:, 0:1]
    raised = per_head[owner_core, pl.ds(2 * mine + 1, 1), :][:, 0:1] * LOG2E

    def partial(b, m, start, stop, lifted):
        scores = (
            lax.dot_general(
                queries[b, :, m * half : (m + 1) * half],
                keys_values[start:stop, m * half : (m + 1) * half],
                (((1,), (1,)), ((), ())),
                preferred_element_type=jnp.float32,
            )
            * factor
        )
        if lifted:
            scores = jnp.concatenate([scores[:, :lifted] + raised, scores[:, lifted:]], axis=1)
        peak = jnp.max(scores, axis=1, keepdims=True)
        weights = jnp.exp2(scores - peak)
        sums = jnp.sum(weights, axis=1, keepdims=True)
        found = jnp.dot(
            weights.astype(jnp.bfloat16),
            keys_values[start:stop, head:],
            preferred_element_type=jnp.float32,
        )
        return peak, sums, found

    def wait_queries(b):
        for others in (plane - 1, plane):

            @pl.when(is_owner if others < plane else jnp.logical_not(is_owner))
            def _():
                place = queries.at[b, : others * rows]
                remote(place, place, q_send.at[0], q_recv.at[b], tp=twin).wait_recv()

    def begin(b):
        wait_queries(b)
        for m in range(2):
            peak, sums, found = partial(b, m, 0, most, ctx_total)
            held_peak[m] = jnp.broadcast_to(peak, (tile, LANES))
            held_sums[m] = jnp.broadcast_to(sums, (tile, LANES))
            held[m] = found

    def finish(b):
        outs = []
        for m in range(2):
            peak, sums, found = partial(b, m, most, keys_values.shape[0], 0)
            old_peak = held_peak[m][:, 0:1]
            top = jnp.maximum(peak, old_peak)
            now = jnp.exp2(peak - top)
            before = jnp.exp2(old_peak - top)
            sums = sums * now + held_sums[m][:, 0:1] * before
            outs.append((found * now + held[m] * before) / sums)
        hand_back(b, outs)

    def whole(b):
        wait_queries(b)
        outs = []
        for m in range(2):
            _, sums, found = partial(b, m, 0, keys_values.shape[0], ctx_total)
            outs.append(found / sums)
        hand_back(b, outs)

    def hand_back(b, outs):
        diff = outs[0] - weight_of_second * outs[1]
        mean = jnp.sum(diff * diff, axis=1, keepdims=True) * (1.0 / head)
        out_stage[b, :, :] = (diff * lax.rsqrt(mean + EPSILON) * gain[...]).astype(jnp.bfloat16)
        for k in range(1, plane):
            out_copy(b, k, my_head).start()
        attended[b, my_head] = out_stage[b, aligned(my_head * rows, rows, ROWS), :]

    forward_all(half_way, jnp.maximum(half_way, far * parts))
    process(farthest, "half", chips, half_rows)
    pass_on("half", chips - 1)
    take("context", slots - 1)

    def take_block(i, carry):
        take("block", i)
        return carry

    lax.fori_loop(0, chips - 1, take_block, 0)
    take("half", chips - 1)
    begin(block_of(swap(0)))
    pass_on("half", chips)
    take("half", chips)
    finish(block_of(swap(0)))
    weight_copy(1 - c).wait_recv()
    later_loads[7].wait()

    sizes = (kept // 2, (width - kept) // 2)

    def columns(kind, n):
        start = n * sizes[0] if kind == 0 else kept + (n - 2) * sizes[1]
        return aligned(start, sizes[kind], LANES)

    def right_copy(b, kind, n):
        cols = columns(kind, n)
        return remote(
            stage.at[b, :, cols],
            incoming.at[b + 1, :, cols],
            stage_sem.at[0],
            sums_sem.at[(b + 1) * UNITS + n],
            tp=t + 2,
        )

    def left_copy(b, kind, n):
        cols = columns(kind, n)
        return remote(
            stage.at[b, :, cols],
            incoming.at[b, :, cols],
            stage_sem.at[0],
            sums_sem.at[b * UNITS + n],
            tp=t - 2,
        )

    def rows_of(ref, b):
        return jnp.concatenate([ref[b, g] for g in range(plane)], axis=1)

    def borrowed(b, n):
        if isinstance(n, int):
            if n == 2:
                lend_block(b).wait_recv()
        else:

            @pl.when(n == 2)
            def _():
                lend_block(b).wait_recv()

        return jnp.dot(
            rows_of(lent_blocks, b),
            mod_weight[: 2 * local, aligned((n - 2) * sizes[1], sizes[1], LANES)],
            preferred_element_type=jnp.float32,
        )

    def unit_at(q):
        index, n = lax.div(q, UNITS), lax.rem(q, UNITS)
        n = jnp.where(n == 0, 2, jnp.where(n == 3, 3, n - 1))
        for place, (i, piece_of) in enumerate(
            [(0, 0), (1, 2), (1, 0), (1, 1), (1, 3), (0, 2), (0, 1), (0, 3)]
        ):
            index = jnp.where(q == place, i, index)
            n = jnp.where(q == place, piece_of, n)
        return swap(index), n

    def send_sums(b, n):
        @pl.when(z == 0)
        def _():
            right_copy(b, 0, n).start()

        @pl.when(z > 0)
        def _():
            left_copy(b, 0, n).start()

    def project(i):
        b = block_of(swap(i))
        place = attended.at[b, : plane - 1]
        remote(place, place, out_send.at[1], out_recv.at[b], tp=twin).wait_recv()
        sends = at_end & (b != z)

        @pl.when(sends)
        def _():
            lend_block(b).start()

        x = rows_of(attended, b)
        for n in range(UNITS):
            kind = n // 2
            start = n * sizes[0] if kind == 0 else kept + (n - 2) * sizes[1]
            cols = slice(start, start + sizes[kind])

            def find():
                return jnp.dot(x, weight[:, cols], preferred_element_type=jnp.float32)

            if kind == 0:
                found = find()
                own[b, :, cols] = found

                @pl.when(sends)
                def _():
                    stage[b, :, cols] = found.astype(jnp.bfloat16)

                    @pl.when((i > 0) | (n == 0))
                    def _():
                        send_sums(b, n)
            else:

                @pl.when(jnp.logical_not(sends))
                def _():
                    own[b, :, cols] = find()

        @pl.when(at_end & (i == 1))
        def _():
            send_sums(block_of(swap(0)), 1)

    hop = 2

    def combine_one(b, n, wanted_here, copy, slot, neighbour):
        for kind in range(2):
            cols = columns(kind, n)
            here = wanted_here & (lax.div(n, 2) == kind)
            received = here & jnp.logical_not(neighbour) if kind else here

            @pl.when(received)
            def _():
                copy(b, kind, n).wait_recv()
                stage[b, :, cols] = (
                    own[b, :, cols] + incoming[slot, :, cols].astype(jnp.float32)
                ).astype(jnp.bfloat16)
                copy(b, kind, n).start()

            if kind:

                @pl.when(here & neighbour)
                def _():
                    stage[b, :, cols] = (own[b, :, cols] + borrowed(b, n)).astype(jnp.bfloat16)
                    copy(b, kind, n).start()

    def combine_step(i, carry):
        q = jnp.maximum(i - hop * (chips - 1 - z), 0)
        b, n = unit_at(q)
        here = (i >= hop * (chips - 1 - z)) & (b < z)
        combine_one(b, n, here, left_copy, b, z + 2 == chips)
        p = jnp.maximum(i - hop * z, 0)
        e, n = unit_at(p)
        e = chips - 1 - e
        here = (i >= hop * z) & (e > z)
        combine_one(e, n, here, right_copy, e + 1, z == 1)
        return carry

    def combine(start, stop):
        @pl.when(jnp.logical_not(at_end))
        def _():
            lax.fori_loop(start, stop, combine_step, 0)

    steps = 2 * chips - 1

    def attend_step(k, carry):
        index = lax.div(k, 2)
        attends = (lax.rem(k, 2) == 0) & (k + 1 < steps)

        @pl.when(attends)
        def _():
            whole(block_of(swap(index + 1)))

        @pl.when(jnp.logical_not(attends))
        def _():
            project(index)

        @pl.when((k == 3) & by_end)
        def _():
            lend.wait_recv()
            lend_across(c).start()

        @pl.when(k == steps - 3)
        def _():
            combine(0, hop + 1)

        @pl.when((k == steps - 2) & by_end)
        def _():
            lend_across(1 - c).wait_recv()

        @pl.when(k == steps - 2)
        def _():
            combine(hop + 1, hop + 2)

        return carry

    lax.fori_loop(0, steps, attend_step, 0)

    def copies_left():
        for k in range(1, plane):
            remote(
                attended.at[:, 0], attended.at[:, 0], out_send.at[k], out_recv.at[0], tp=twin
            ).wait_send()

        def sent_tokens(b, carry):
            place = tokens.at[aligned(b * rows, rows, ROWS)]

            @pl.when((b <= z) & (z + 1 < chips))
            def _():
                remote(place, place, tok_send.at[0, b], tok_recv.at[0], tp=twin).wait_send()

            @pl.when((b >= z) & (z > 0))
            def _():
                remote(place, place, tok_send.at[1, b], tok_recv.at[0], tp=twin).wait_send()

            return carry

        lax.fori_loop(0, chips, sent_tokens, 0)
        place = tokens.at[: chips * rows]
        remote(place, place, tok_send.at[2, 0], tok_recv.at[0], tp=twin).wait_send()
        for g in range(heads):
            place = q_stage.at[g, : chips * rows]
            remote(place, place, q_send.at[2 * g + 1], q_recv.at[0], tp=twin).wait_send()

            @pl.when(c * heads + g != my_head)
            def _():
                remote(place, place, q_send.at[2 * g], q_recv.at[0], tp=twin).wait_send()

        for k in range(1, sp_size):

            @pl.when(wanted(k))
            def _():
                place = kv_stage.at[0]
                remote(place, place, kv_send.at[k], kv_recv.at[0], tp=twin).wait_send()

        @pl.when(is_owner)
        def _():
            remote(
                keys_values, keys_values, kv_twin.at[0], kv_pass.at[0], tp=twin
            ).wait_send()

        place = mod_parts.at[: sp_size - 1]
        remote(place, place, part_send, part_recv, tp=twin).wait_send()
        place = mod_pieces.at[: tp_size - 1]
        remote(place, place, piece_send, piece_recv.at[0], tp=twin).wait_send()
        head_copy(c).wait_send()
        weight_copy(c).wait_send()

    copies_left()
    combine(hop + 2, (chips - 1) * (UNITS + hop))

    for n in range(UNITS):
        kind = n // 2
        start = n * sizes[0] if kind == 0 else kept + (n - 2) * sizes[1]
        cols = slice(start, start + sizes[kind])

        def add(copy, slot, present, neighbour):
            received = present & jnp.logical_not(neighbour) if kind else present

            @pl.when(received)
            def _():
                copy(z, kind, n).wait_recv()
                own[z, :, cols] = own[z, :, cols] + incoming[slot, :, cols].astype(jnp.float32)

            if kind:

                @pl.when(neighbour)
                def _():
                    own[z, :, cols] = own[z, :, cols] + borrowed(z, n)

        add(right_copy, z + 1, z > 0, z == 1)
        add(left_copy, z, z + 1 < chips, z + 2 == chips)
        result[:, cols] = (
            tokens[aligned(t * rows, rows, ROWS), cols].astype(jnp.float32)
            + mod_rows[4:5, cols] * own[z, :, cols]
        ).astype(jnp.bfloat16)

    @pl.when(at_end)
    def _():
        place = stage.at[: chips - 1, :, :kept]
        remote(place, place, stage_sem.at[0], sums_sem.at[0], tp=twin).wait_send()
        lend.wait_send()
        place = attended.at[: chips - 1]
        remote(place, place, lend_send.at[2], block_recv.at[0], tp=twin).wait_send()

    @pl.when(jnp.logical_not(at_end))
    def _():
        place = stage.at[: chips - 1]
        remote(place, place, stage_sem.at[0], sums_sem.at[0], tp=twin).wait_send()

    @pl.when(by_end)
    def _():
        lend_across(c).wait_send()


def kept_of(width):
    return width * 5 // 8


def tables(grid_rows, half):
    quarter = half // 4
    inverse = (ROPE_BASE ** (-np.arange(quarter) / quarter)).astype(np.float32)
    sign = np.where(np.arange(half) % (2 * quarter) < quarter, -1.0, 1.0)
    places = np.concatenate([np.arange(grid_rows), np.arange(GRID_W)]).astype(np.float32)
    angles = (places[:, None] * np.tile(inverse, 4)).astype(np.float64)
    return np.stack([np.cos(angles), np.sin(angles) * sign]).astype(np.float32)


def row(x):
    return x.reshape(1, -1) if x.size > 1 else jnp.broadcast_to(x.reshape(1, 1), (1, LANES))


def shards(
    sp_size,
    tp_size,
    latent,
    context,
    condition,
    context_condition,
    modulation,
    query_weight,
    key_weight,
    value_weight,
    lambdas,
    context_lift,
    head_gain,
    output_weight,
):
    rows, width = latent.shape
    chips = tp_size // 2
    local = query_weight.shape[1]
    heads = lambdas.shape[0]
    head = local // heads
    half = head // 2
    plane = 2 * heads
    block_tokens = rows * tp_size
    ctx_rows = context.shape[0]
    piece = modulation.shape[2]
    depth = modulation.shape[1]
    parts = rows // ROWS
    table = tables(sp_size * block_tokens // GRID_W, half)
    vmem = pl.BlockSpec(memory_space=pltpu.VMEM)
    anywhere = pl.BlockSpec(memory_space=pltpu.HBM)
    bf16, f32 = jnp.bfloat16, jnp.float32
    dma = pltpu.SemaphoreType.DMA
    blocks = (chips, rows, width)
    return pl.pallas_call(
        functools.partial(block_kernel, sp_size, tp_size),
        out_shape=jax.ShapeDtypeStruct((rows, width), bf16),
        in_specs=[anywhere] * 13,
        out_specs=vmem,
        scratch_shapes=[
            pltpu.VMEM((block_tokens, width), bf16),
            pltpu.VMEM(context.shape, bf16),
            pltpu.VMEM((max(2 * rows, ctx_rows), width), bf16),
            pltpu.VMEM((max(depth, 2 * local), max(3 * piece, width - kept_of(width))), bf16),
            pltpu.VMEM((width, local), bf16),
            pltpu.VMEM((width, local), bf16),
            pltpu.VMEM((width, local), bf16),
            pltpu.VMEM((2 * local, width), bf16),
            pltpu.VMEM((sp_size * (ctx_rows + block_tokens), 2 * head), bf16),
            pltpu.VMEM((chips, plane * rows, head), bf16),
            pltpu.VMEM((heads, block_tokens + ctx_rows, 2 * head), bf16),
            pltpu.VMEM((heads, block_tokens, head), bf16),
            pltpu.VMEM((chips, plane * rows, head), bf16),
            pltpu.VMEM((chips, plane, rows, head), bf16),
            pltpu.VMEM(blocks, f32),
            pltpu.VMEM(blocks, bf16),
            pltpu.VMEM((chips + 1, rows, width), bf16),
            pltpu.VMEM((chips, plane, rows, head), bf16),
            pltpu.VMEM((sp_size, 8, piece), f32),
            pltpu.VMEM((tp_size, 8, piece), f32),
            pltpu.VMEM((8, width), f32),
            pltpu.VMEM((2, depth), f32),
            pltpu.VMEM(table.shape, f32),
            pltpu.VMEM((block_tokens, half), f32),
            pltpu.VMEM((block_tokens, half), f32),
            pltpu.VMEM((1, head), f32),
            pltpu.VMEM((2, 8, LANES), f32),
            pltpu.VMEM((2,) + row(lambdas).shape, f32),
            pltpu.VMEM((2, plane * rows, head), f32),
            pltpu.VMEM((2, plane * rows, LANES), f32),
            pltpu.VMEM((2, plane * rows, LANES), f32),
            dma((15,)),
            dma((3, chips)),
            dma((parts * chips,)),
            dma((2 * chips,)),
            dma(()),
            dma(()),
            dma(()),
            dma((tp_size,)),
            dma((sp_size,)),
            dma((1,)),
            dma((chips + 2,)),
            dma((chips + 2,)),
            dma((2 * heads,)),
            dma((chips,)),
            dma((plane,)),
            dma((chips,)),
            dma((2,)),
            dma((2,)),
            dma((1,)),
            dma((UNITS * (chips + 1),)),
            dma((3,)),
            dma((2,)),
            dma((chips,)),
        ],
        compiler_params=pltpu.CompilerParams(
            collective_id=0, has_side_effects=True, vmem_limit_bytes=VMEM_LIMIT
        ),
        name="block",
    )(
        *(
            pltpu.with_memory_space_constraint(x, pltpu.HBM)
            for x in (
                latent,
                context,
                row(condition),
                row(context_condition),
                modulation,
                query_weight,
                key_weight,
                value_weight,
                table,
                row(lambdas),
                row(context_lift),
                row(head_gain),
                output_weight,
            )
        )
    )


def solution(mesh):
    in_specs = (
        P(("sp", "tp"), None),
        P("sp", None),
        P(),
        P(),
        P(None, "sp", "tp"),
        P(None, "tp"),
        P(None, "tp"),
        P(None, "tp"),
        P("tp"),
        P("tp"),
        P(),
        P("tp", None),
    )
    out_specs = P(("sp", "tp"), None)
    body = functools.partial(shards, mesh.shape["sp"], mesh.shape["tp"])
    return jax.shard_map(body, mesh=mesh, in_specs=in_specs, out_specs=out_specs, check_vma=False)
```
